128 devices in a mesh: sp: 32 (over z, y, core), tp: 4 (over x).
Axes of the slice: x: 4, y: 4, z: 4, core: 2. Of those that a mesh axis runs over, the one named last changes fastest.
Arguments:
- out_grad: bfloat16 [4096, 2048], P('sp', 'tp'), may hold values from -6 to 6
- route_ids: int32 [4096, 2], P('sp'), may hold values from 0 to 31, as said below
- route_weight: float32 [4096, 2], P('sp'), may hold values from 0.1 to 0.9
- expert_inputs: bfloat16 [32, 512, 2048], P('sp'), may hold values from -6 to 6
- gate_weight: bfloat16 [32, 2048, 3072], P('sp', None, 'tp'), may hold values from -0.125 to 0.125
- up_weight: bfloat16 [32, 2048, 3072], P('sp', None, 'tp'), may hold values from -0.125 to 0.125
- down_weight: bfloat16 [32, 3072, 2048], P('sp', 'tp'), may hold values from -0.109375 to 0.109375
- out_gate: bfloat16 [4096, 2048], P('sp', 'tp'), may hold values from -6 to 6
- in_gate: bfloat16 [4096, 2048], P('sp', 'tp'), may hold values from -6 to 6
- values: bfloat16 [4096, 2048], P('sp', 'tp'), may hold values from -6 to 6
- conv_out: bfloat16 [4096, 2048], P('sp', 'tp'), may hold values from -6 to 6
- conv_taps: bfloat16 [3, 2048], P(None, 'tp'), may hold values from -3.5 to 3.5
- proj_weight: bfloat16 [2048, 2048], P(None, 'tp'), may hold values from -0.125 to 0.125
Outputs:
- resid_grad: bfloat16 [4096, 2048], P('sp', 'tp')
- out_gate_grad: bfloat16 [4096, 2048], P('sp', 'tp')
- in_gate_grad: bfloat16 [4096, 2048], P('sp', 'tp')
- values_grad: bfloat16 [4096, 2048], P('sp', 'tp')
- proj_grad: float32 [2048, 2048], P('sp', 'tp')
- gate_grad: bfloat16 [32, 2048, 3072], P('sp', None, 'tp')
- up_grad: bfloat16 [32, 2048, 3072], P('sp', None, 'tp')
- down_grad: bfloat16 [32, 3072, 2048], P('sp', 'tp')
The draws below stay inside these ranges and needn't reach their ends.
Inputs may be any that keep to these rules, and one draw needn't show every extreme that they name: `route_ids`: each row names two different experts. Among the rows of one device (aligned blocks of 128 rows) no expert is named more than 16 times, and in every draw one expert is named exactly 16 times in every block.
All inputs are finite; a program needn't handle non-finite values.
Results may differ from the reference program's by a relative error of at most 0.017.
Values may be sent and summed in bfloat16 or wider, within the bound.
A program may use at most 128 MiB of HBM per device.

```python
import math
import jax
import jax.numpy as jnp
from jax import lax

D = 2048
FF = 3072
TAPS = 3
TOK_DEV = 128
TOKENS = 4096
EXPERTS = 32
CAP = 16
SLOTS = 512
N_TP = 4


def draw_route_ids(key, part):
    blocks = TOKENS // TOK_DEV
    tickets = jnp.arange(EXPERTS * CAP, dtype=jnp.int32) // CAP
    filled = jax.random.randint(jax.random.fold_in(key, 11), (), 0, EXPERTS)

    def one_block(block_key):
        extra = jax.random.randint(jax.random.fold_in(block_key, 1), (), 0, EXPERTS)
        shuffled = tickets[jax.random.permutation(jax.random.fold_in(block_key, 2), EXPERTS * CAP)]
        priority = jnp.where(shuffled == filled, 0, jnp.where(shuffled == extra, 1, 2)).astype(jnp.int32)
        chosen = shuffled[jnp.argsort(priority, stable=True)][:2 * TOK_DEV]
        ordered = jnp.sort(chosen)
        pairs = jnp.stack([ordered[:TOK_DEV], ordered[TOK_DEV:]], axis=1)
        flips = jax.random.randint(jax.random.fold_in(block_key, 3), (TOK_DEV, 1), 0, 2)
        pairs = jnp.where(flips == 1, pairs[:, ::-1], pairs)
        shuffle_rows = jax.random.permutation(jax.random.fold_in(block_key, 4), TOK_DEV)
        return pairs[shuffle_rows]
    block_keys = jax.random.split(jax.random.fold_in(key, 7), blocks)
    return jax.vmap(one_block)(block_keys).reshape(TOKENS, 2).astype(jnp.int32)


def spiked(values, key, source, target, blocks, factor):
    def block_of(position):
        return (jnp.arange(values.shape[position]) // (values.shape[position] // blocks)).reshape((-1,) + (1,) * (values.ndim - 1 - position))

    first = jax.random.permutation(key, blocks)[block_of(target)]
    other_side = (block_of(target) + blocks // 2) % blocks
    return jnp.where((block_of(source) == first) | (block_of(source) == other_side), factor * values, values)


def levels(rng, extent, pieces, least, largest):
    level, own = 1.0, jax.random.fold_in(rng, 6)
    for axis_at, parts in pieces:
        heights = jnp.exp(jax.random.uniform(jax.random.fold_in(own, axis_at), (parts,), jnp.float32, least / len(pieces), largest / len(pieces)))
        level = level * jnp.repeat(heights, extent[axis_at] // parts).reshape([-1 if axis == axis_at else 1 for axis in range(len(extent))])
    return level


def centred(own_key, dims, deviation, reach, cuts=(), held_as=jnp.bfloat16):
    level = levels(own_key, dims, cuts, -0.22, 0.18) if cuts else 1.0
    entries = jax.random.normal(own_key, dims, jnp.float32) * deviation * level
    return jnp.minimum(jnp.maximum(entries, -reach), reach).astype(held_as)


def bell_draw_with(own_key, shape, scale, bound, shards, heavy, kind=jnp.bfloat16):
    values = scale * jax.random.normal(own_key, shape, jnp.float32)
    if shards:
        values = values * levels(own_key, shape, shards, -0.22, 0.18)
    return jnp.clip(spiked(values, jax.random.fold_in(own_key, 3), *heavy), -bound, bound).astype(kind)


def setup_inputs(seed: int = 0) -> dict:
    streams_of = jax.random.split(jax.random.key(seed), 14)
    out_grad = bell_draw_with(streams_of[0], (TOKENS, D), 1.0, 6.0, ((0, 32), (1, 4)), (0, 1, 32, 2.75))
    route_ids = draw_route_ids(jax.random.fold_in(streams_of[13], 71), 0)
    route_weight = jnp.clip(0.1 + 0.79999997 * jax.random.uniform(streams_of[2], (TOKENS, 2), jnp.float32) ** levels(streams_of[2], (TOKENS, 2), ((0, 32),), -0.2, 0.2), 0.1, 0.9)
    expert_inputs = centred(streams_of[3], (EXPERTS, SLOTS, D), 1.0, 6.0, ((0, 32),))
    gate_weight = centred(streams_of[4], (EXPERTS, D, FF), D ** -0.5, 0.125, ((0, 32), (2, 4)))
    up_weight = centred(streams_of[5], (EXPERTS, D, FF), D ** -0.5, 0.125, ((0, 32), (2, 4)))
    down_weight = centred(streams_of[6], (EXPERTS, FF, D), FF ** -0.5, 0.109375, ((0, 32), (1, 4)))
    out_gate = centred(streams_of[7], (TOKENS, D), 1.0, 6.0, ((0, 32), (1, 4)))
    in_gate = centred(streams_of[8], (TOKENS, D), 1.0, 6.0, ((0, 32), (1, 4)))
    values = centred(streams_of[9], (TOKENS, D), 1.0, 6.0, ((0, 32), (1, 4)))
    conv_out = centred(streams_of[10], (TOKENS, D), 1.0, 6.0, ((0, 32), (1, 4)))
    conv_taps = centred(streams_of[11], (TAPS, D), TAPS ** -0.5, 3.5, ((1, 4),))
    proj_weight = centred(streams_of[12], (D, D), D ** -0.5, 0.125, ((1, 4),))
    return dict(out_grad=out_grad, route_ids=route_ids, route_weight=route_weight, expert_inputs=expert_inputs, gate_weight=gate_weight, up_weight=up_weight, down_weight=down_weight, out_gate=out_gate, in_gate=in_gate, values=values, conv_out=conv_out, conv_taps=conv_taps, proj_weight=proj_weight)


def slot_rows(route_ids):
    blocks = route_ids.reshape(TOKENS // TOK_DEV, 2 * TOK_DEV)
    onehot = (blocks[:, :, None] == jnp.arange(EXPERTS, dtype=jnp.int32)[None, None, :]).astype(jnp.int32)
    ranked = lax.optimization_barrier(jnp.sum((jnp.cumsum(onehot, axis=1) - onehot) * onehot, axis=2))
    source = jnp.arange(TOKENS // TOK_DEV, dtype=jnp.int32)[:, None]
    return (blocks * SLOTS + source * CAP + ranked).reshape(-1).astype(jnp.int32)

def expert_step(operands):
    inputs, routed, gate_w, up_w, down_w = operands
    pre_gate = jnp.dot(inputs, gate_w, preferred_element_type=jnp.float32)
    pre_up = jnp.dot(inputs, up_w, preferred_element_type=jnp.float32)
    sigmoid_g = jax.nn.sigmoid(pre_gate)
    activated = pre_gate * sigmoid_g
    hidden = (activated * pre_up).astype(jnp.bfloat16)
    d_hidden = jnp.dot(routed, down_w.T, preferred_element_type=jnp.float32)
    d_gate = (d_hidden * pre_up * sigmoid_g * (1.0 + pre_gate * (1.0 - sigmoid_g))).astype(jnp.bfloat16)
    d_up = (d_hidden * activated).astype(jnp.bfloat16)
    slot_scale = 1.0 / math.sqrt(SLOTS)
    gate_grad = (jnp.dot(inputs.T, d_gate, preferred_element_type=jnp.float32) * slot_scale).astype(jnp.bfloat16)
    up_grad = (jnp.dot(inputs.T, d_up, preferred_element_type=jnp.float32) * slot_scale).astype(jnp.bfloat16)
    down_grad = (jnp.dot(hidden.T, routed, preferred_element_type=jnp.float32) * slot_scale).astype(jnp.bfloat16)
    block_width = FF // N_TP
    back = jnp.zeros((SLOTS, D), jnp.float32)
    for block in range(N_TP):
        lower = block * block_width
        upper = lower + block_width
        part_sum = jnp.dot(lax.slice_in_dim(d_gate, lower, upper, axis=1), lax.slice_in_dim(gate_w, lower, upper, axis=1).T, preferred_element_type=jnp.float32)
        part_sum = part_sum + jnp.dot(lax.slice_in_dim(d_up, lower, upper, axis=1), lax.slice_in_dim(up_w, lower, upper, axis=1).T, preferred_element_type=jnp.float32)
        back = back + lax.optimization_barrier(part_sum.astype(jnp.bfloat16)).astype(jnp.float32)
    return (gate_grad, up_grad, down_grad, back.astype(jnp.bfloat16))

def reference(out_grad, route_ids, route_weight, expert_inputs, gate_weight, up_weight, down_weight, out_gate, in_gate, values, conv_out, conv_taps, proj_weight):
    rows = slot_rows(route_ids)
    weighted = (route_weight[:, :, None] * out_grad.astype(jnp.float32)[:, None, :]).astype(jnp.bfloat16).reshape(2 * TOKENS, D)
    routed = jnp.zeros((EXPERTS * SLOTS, D), jnp.bfloat16).at[rows].set(weighted).reshape(EXPERTS, SLOTS, D)
    gate_grad, up_grad, down_grad, back = lax.map(expert_step, (expert_inputs, routed, gate_weight, up_weight, down_weight))
    pair_back = back.reshape(EXPERTS * SLOTS, D)[rows].astype(jnp.float32).reshape(TOKENS, 2, D)
    resid_grad = (out_grad.astype(jnp.float32) + pair_back[:, 0] + pair_back[:, 1]).astype(jnp.bfloat16)
    gate_vals = out_gate.astype(jnp.float32)
    conv_vals = conv_out.astype(jnp.float32)
    mixed_in = (gate_vals * conv_vals).astype(jnp.bfloat16)
    proj_grad = jnp.dot(resid_grad.T, mixed_in, preferred_element_type=jnp.float32) * (1.0 / math.sqrt(TOKENS))
    mix_grad = jnp.dot(resid_grad, proj_weight, preferred_element_type=jnp.float32)
    out_gate_grad = (mix_grad * conv_vals).astype(jnp.bfloat16)
    conv_grad = lax.optimization_barrier((mix_grad * gate_vals).astype(jnp.bfloat16)).astype(jnp.float32)
    padded = jnp.pad(conv_grad, ((1, 1), (0, 0)))
    tap_vals = conv_taps.astype(jnp.float32)
    value_grad = padded[2:] * tap_vals[0] + padded[1:-1] * tap_vals[1] + padded[:-2] * tap_vals[2]
    in_gate_grad = (value_grad * values.astype(jnp.float32)).astype(jnp.bfloat16)
    values_grad = (value_grad * in_gate.astype(jnp.float32)).astype(jnp.bfloat16)
    return (resid_grad, out_gate_grad, in_gate_grad, values_grad, proj_grad, gate_grad, up_grad, down_grad)
```

```python
import functools
import math

import jax
import jax.numpy as jnp
from jax import lax
from jax.experimental import pallas as pl
from jax.experimental.pallas import tpu as pltpu
from jax.sharding import PartitionSpec as P

MESH = pl.DeviceIdType.MESH
BF = jnp.bfloat16
F32 = jnp.float32

Z, Y, C = 4, 4, 2
SP = Z * Y * C
TP = 4
TOK = 128
CAP = 16
SLOTS = SP * CAP
CH = 512
HID = 768
ROWS = 64
GROUP = Y * C
CHUNK = GROUP * CAP
ORDER = (0, 1, 3, 2)


def mm(a, b, dims):
    return lax.dot_general(a, b, ((dims[:1], dims[1:]), ((), ())), preferred_element_type=F32)


def at(block, size):
    return pl.ds(pl.multiple_of(block * size, size), size)


def layer_kernel(
    ids_hbm, w_hbm, og_hbm, inp_hbm, gw_hbm, uw_hbm, dw_hbm,
    gate_hbm, ing_hbm, val_hbm, conv_hbm, taps_hbm, pw_hbm,
    resid_out, ogg_out, igg_out, vg_out, proj_out, routed_out, hid_out, dgu_out,
    ids_v, w_v, og_v, inp_v, gu_v, dw_v, gate_v, ing_v, val_v, conv_v, taps_v, pw_v,
    ogopp_v, disp_v, wslot_v, out0_v, out2_v, r_v, s_v, a_v, hid_v, dgu_v,
    p_v, rp_v, b0_v, ret0_v, ret2_v, m2_v, r2_v, rf_v, resid_v, cg_v, before_v, after_v,
    ogg_v, igg_v, vg_v, z_v, pp_v, pair_v, q_v, rq_v, proj_v,
    ld_sem, st_sem, ogopp_sem, disp_sem, recv0_sem, recv2_sem, x_send, x_recv,
    pn_send, pn_recv, ret_send, ret_recv, m2_sem, rf_send, rf_recv, halo_sem, pair_sem,
    rq_send, rq_recv,
):
    sp = lax.axis_index("sp")
    x = lax.axis_index("tp")
    z = sp // GROUP
    inner = lax.rem(sp, GROUP)
    core = lax.rem(sp, C)
    chip = sp // C
    xp, xm, xo = lax.rem(x + 1, TP), lax.rem(x + 3, TP), lax.rem(x + 2, TP)

    def load(i, src, dst):
        copy = pltpu.make_async_copy(src, dst, ld_sem.at[i])
        copy.start()
        return copy

    loads = [
        load(0, ids_hbm, ids_v),
        load(1, w_hbm, w_v),
        load(2, og_hbm, og_v),
        load(3, inp_hbm, inp_v),
        load(4, gw_hbm, gu_v.at[:, pl.ds(0, HID)]),
        load(5, uw_hbm, gu_v.at[:, pl.ds(HID, HID)]),
        load(6, dw_hbm, dw_v),
        load(7, gate_hbm, gate_v),
        load(8, conv_hbm, conv_v),
        load(9, pw_hbm, pw_v),
        load(10, ing_hbm, ing_v),
        load(11, val_hbm, val_v),
        load(12, taps_hbm, taps_v),
    ]

    barrier = pltpu.get_barrier_semaphore()

    def greet(i, carry):
        other = lax.rem(sp + 1 + i, SP)
        pl.semaphore_signal(barrier, inc=1, device_id=(other, x), device_id_type=MESH)
        return carry

    lax.fori_loop(0, SP - 1, greet, 0)
    for t in (xp, xm, xo):
        pl.semaphore_signal(barrier, inc=1, device_id=(sp, t), device_id_type=MESH)

    loads[0].wait()
    loads[1].wait()
    loads[2].wait()
    ids = ids_v[...]
    wts = w_v[...]
    e_iota = lax.broadcasted_iota(jnp.int32, (SP, TOK), 0)
    first = e_iota == ids[0:1, :]
    second = e_iota == ids[1:2, :]
    named = jnp.where(first | second, 1.0, 0.0)
    w_et = jnp.where(first, wts[0:1, :], 0.0) + jnp.where(second, wts[1:2, :], 0.0)
    earlier = lax.broadcasted_iota(jnp.int32, (TOK, TOK), 0) < lax.broadcasted_iota(
        jnp.int32, (TOK, TOK), 1
    )
    prefix = mm(named.astype(BF), jnp.where(earlier, 1.0, 0.0).astype(BF), (1, 0))
    rank = jnp.where(named > 0.5, prefix, -1.0)
    r_iota = lax.broadcasted_iota(jnp.int32, (SP, CAP, TOK), 1).astype(F32)
    hit = jnp.broadcast_to(rank[:, None, :], (SP, CAP, TOK)) == r_iota
    disp = jnp.where(hit, 1.0, 0.0)
    wslot = jnp.sum(disp * w_et[:, None, :], axis=2, keepdims=True)
    disp_v[...] = disp.reshape(SLOTS, TOK).astype(BF)
    wslot_v[...] = jnp.broadcast_to(wslot, (SP, CAP, TOK)).reshape(SLOTS, TOK)

    def dispatch(tok_ref, out_ref):
        rows = mm(disp_v[...], tok_ref[...], (1, 0))
        out_ref[...] = (rows * jnp.tile(wslot_v[...], (1, CH // TOK))).astype(BF)

    dispatch(og_v, out0_v)
    pl.semaphore_wait(barrier, SP - 1 + TP - 1)

    ogopp = pltpu.make_async_remote_copy(
        og_v, ogopp_v, ogopp_sem.at[0], ogopp_sem.at[1], device_id=(sp, xo), device_id_type=MESH
    )
    ogopp.start()

    def scatter(out_ref, block, which, recv_sem):
        r_v[block, at(sp, CAP), :] = out_ref[at(sp, CAP), :]
        for dz in ORDER:
            home = lax.rem(z - dz + Z, Z) * GROUP

            def send(i, carry):
                there = home + (lax.rem(inner + 1 + i, GROUP) if dz == 0 else lax.rem(inner + i, GROUP))
                pltpu.make_async_remote_copy(
                    out_ref.at[at(there, CAP), :],
                    r_v.at[block, at(sp, CAP), :],
                    disp_sem.at[which],
                    recv_sem.at[dz],
                    device_id=(there, x),
                    device_id_type=MESH,
                ).start()
                return carry

            lax.fori_loop(0, GROUP - 1 if dz == 0 else GROUP, send, 0)

    def await_bytes(ref, sem):
        pltpu.make_async_copy(ref, ref, sem).wait()

    def chunk_rows(dz):
        return at(lax.rem(z + dz, Z), CHUNK)

    scatter(out0_v, 0, 0, recv0_sem)

    x_copies = []

    def await_group(block, dz, recv_sem):
        count = CHUNK - CAP if dz == 0 else CHUNK
        await_bytes(r_v.at[block, pl.ds(0, count), :], recv_sem.at[dz])

    def forward(k):
        dz = ORDER[k]
        await_group(0, dz, recv0_sem)
        for way, (there, landing) in enumerate(((xp, 3), (xm, 1))):
            copy = pltpu.make_async_remote_copy(
                r_v.at[0, chunk_rows(dz), :],
                r_v.at[landing, chunk_rows(dz), :],
                x_send.at[way, k],
                x_recv.at[way, k],
                device_id=(sp, there),
                device_id_type=MESH,
            )
            copy.start()
            x_copies.append(copy)

    TILE = 256

    def hidden_tile(n):
        cols = slice(n * TILE, (n + 1) * TILE)
        ups = slice(HID + n * TILE, HID + (n + 1) * TILE)

        def rows_of(m, carry):
            rows = at(m, 256)
            pre_gate = mm(inp_v[rows, :], gu_v[:, cols], (1, 0))
            pre_up = mm(inp_v[rows, :], gu_v[:, ups], (1, 0))
            sig = 1.0 / (1.0 + jnp.exp(-pre_gate))
            act = pre_gate * sig
            s_v[rows, cols] = act
            a_v[rows, cols] = pre_up * sig * (1.0 + pre_gate * (1.0 - sig))
            hid_v[rows, cols] = (act * pre_up).astype(BF)
            return carry

        lax.fori_loop(0, SLOTS // 256, rows_of, 0)

    loads[3].wait()
    loads[4].wait()
    loads[5].wait()
    hidden_tile(0)
    ogopp.wait_recv()
    dispatch(ogopp_v, out2_v)
    scatter(out2_v, 2, 1, recv2_sem)
    forward(0)
    forward(1)
    hidden_tile(1)
    forward(2)
    forward(3)
    hidden_tile(2)
    stores = []

    def store(i, src, dst):
        copy = pltpu.make_async_copy(src, dst, st_sem.at[i])
        copy.start()
        stores.append(copy)

    store(0, hid_v, hid_out)
    loads[6].wait()

    p_copies = {}

    def give_back(src_ref, dst_ref, which, dz):
        home = lax.rem(z + dz, Z) * GROUP
        if dz == 0:
            dst_ref[at(sp, CAP), :] = src_ref[at(sp, CAP), :]

        def send(i, carry):
            there = home + (lax.rem(inner + 1 + i, GROUP) if dz == 0 else lax.rem(inner + i, GROUP))
            pltpu.make_async_remote_copy(
                src_ref.at[at(there, CAP), :],
                dst_ref.at[at(sp, CAP), :],
                ret_send.at[which],
                ret_recv.at[which],
                device_id=(there, x),
                device_id_type=MESH,
            ).start()
            return carry

        lax.fori_loop(0, GROUP - 1 if dz == 0 else GROUP, send, 0)

    def finish_own(k):
        dz = ORDER[k]
        rows = chunk_rows(dz)
        for way in range(2):
            p_copies[way, k].wait_recv()
        total = p_v[0, rows, :].astype(F32) + rp_v[0, rows, :].astype(F32) + rp_v[1, rows, :].astype(F32)
        b0_v[rows, :] = total.astype(BF)
        give_back(b0_v, ret0_v, 0, dz)

    for k, dz in enumerate(ORDER):
        rows = chunk_rows(dz)
        await_group(2, dz, recv2_sem)
        x_copies[2 * k].wait_recv()
        x_copies[2 * k + 1].wait_recv()
        d_hidden = None
        for j in range(TP):
            term = mm(r_v[j, rows, :], dw_v[:, at(lax.rem(x + j, TP), CH)], (1, 1))
            d_hidden = term if d_hidden is None else d_hidden + term
        dgu_v[rows, 0:HID] = (d_hidden * a_v[rows, :]).astype(BF)
        dgu_v[rows, HID : 2 * HID] = (d_hidden * s_v[rows, :]).astype(BF)
        for j in (1, 3, 2, 0):
            part = mm(dgu_v[rows, :], gu_v[at(lax.rem(x + j, TP), CH), :], (1, 1))
            p_v[j, rows, :] = part.astype(BF)
            if j in (1, 3):
                way = 0 if j == 1 else 1
                copy = pltpu.make_async_remote_copy(
                    p_v.at[j, rows, :],
                    rp_v.at[way, rows, :],
                    pn_send.at[way, k],
                    pn_recv.at[way, k],
                    device_id=(sp, xp if j == 1 else xm),
                    device_id_type=MESH,
                )
                copy.start()
                p_copies[way, k] = copy
            if j == 2:
                give_back(p_v.at[2], ret2_v, 1, dz)
        if k > 0:
            finish_own(k - 1)
    finish_own(Z - 1)
    for j in range(TP):
        store(1 + j, r_v.at[j], routed_out.at[lax.rem(x + j, TP)])
    store(5, dgu_v, dgu_out)

    loads[7].wait()
    loads[8].wait()
    gate_vals = gate_v[...].astype(F32)
    conv_vals = conv_v[...].astype(F32)
    z_v[...] = (gate_vals * conv_vals).astype(BF)

    def await_returned(ref, which):
        await_bytes(ref.at[pl.ds(0, SLOTS - CAP), :], ret_recv.at[which])

    await_returned(ret2_v, 1)
    m2_v[...] = mm(disp_v[...], ret2_v[...], (0, 0)).astype(BF)
    m2 = pltpu.make_async_remote_copy(
        m2_v, r2_v, m2_sem.at[0], m2_sem.at[1], device_id=(sp, xo), device_id_type=MESH
    )
    m2.start()
    await_returned(ret0_v, 0)
    own = og_v[...].astype(F32) + mm(disp_v[...], ret0_v[...], (0, 0))
    m2.wait_recv()
    rf_v[0] = (own + r2_v[...].astype(F32)).astype(BF)
    rf_copies = []
    for i, (there, landing) in enumerate(((xp, 3), (xm, 1), (xo, 2))):
        copy = pltpu.make_async_remote_copy(
            rf_v.at[0],
            rf_v.at[landing],
            rf_send.at[i],
            rf_recv.at[i],
            device_id=(sp, there),
            device_id_type=MESH,
        )
        copy.start()
        rf_copies.append(copy)
    store(6, rf_v.at[0], resid_out)
    loads[9].wait()

    def proj_part(j):
        part = mm(rf_v[j], z_v[...], (0, 0)).astype(BF)
        pp_v[at(lax.rem(x + j, TP), Y)] = part.reshape(Y, C, ROWS, CH)

    mix = mm(rf_v[0], pw_v[at(x, CH), :], (1, 0))
    proj_part(0)
    for j, i in ((3, 0), (1, 1), (2, 2)):
        rf_copies[i].wait_recv()
        mix = mix + mm(rf_v[j], pw_v[at(lax.rem(x + j, TP), CH), :], (1, 0))
        proj_part(j)
    partner = sp + 1 - 2 * core
    pair = pltpu.make_async_remote_copy(
        pp_v.at[:, 1 - core],
        pair_v,
        pair_sem.at[0],
        pair_sem.at[1],
        device_id=(partner, x),
        device_id_type=MESH,
    )
    pair.start()
    ogg_v[...] = (mix * conv_vals).astype(BF)
    cg_v[...] = (mix * gate_vals).astype(BF)
    down = pltpu.make_async_remote_copy(
        cg_v.at[pl.ds(0, 16), :], after_v, halo_sem.at[0], halo_sem.at[1],
        device_id=(lax.rem(sp + SP - 1, SP), x), device_id_type=MESH,
    )
    up = pltpu.make_async_remote_copy(
        cg_v.at[pl.ds(TOK - 16, 16), :], before_v, halo_sem.at[2], halo_sem.at[3],
        device_id=(lax.rem(sp + 1, SP), x), device_id_type=MESH,
    )
    down.start()
    up.start()
    store(7, ogg_v, ogg_out)
    pair.wait_recv()

    def add_pair(i, carry):
        total = pp_v[i, core].astype(F32) + pair_v[i].astype(F32)
        q_v[i] = total.astype(BF)
        return carry

    lax.fori_loop(0, Z * Y, add_pair, 0)

    def reduce_send(i, carry):
        there = lax.rem(chip + 1 + i, Z * Y)
        pltpu.make_async_remote_copy(
            q_v.at[there],
            rq_v.at[chip],
            rq_send.at[0],
            rq_recv.at[0],
            device_id=(there * C + core, x),
            device_id_type=MESH,
        ).start()
        return carry

    lax.fori_loop(0, Z * Y - 1, reduce_send, 0)
    rq_v[chip] = q_v[chip]

    loads[10].wait()
    loads[11].wait()
    loads[12].wait()
    down.wait_recv()
    up.wait_recv()
    cg = cg_v[...].astype(F32)
    taps = taps_v[...].astype(F32)
    row = lax.broadcasted_iota(jnp.int32, (TOK, CH), 0)
    has_before = jnp.where(sp > 0, 1.0, 0.0)
    has_after = jnp.where(sp < SP - 1, 1.0, 0.0)
    before = before_v[...].astype(F32)[15:16, :] * has_before
    after = after_v[...].astype(F32)[0:1, :] * has_after
    nxt = jnp.where(row == TOK - 1, jnp.broadcast_to(after, (TOK, CH)), pltpu.roll(cg, TOK - 1, 0))
    prv = jnp.where(row == 0, jnp.broadcast_to(before, (TOK, CH)), pltpu.roll(cg, 1, 0))
    value_grad = nxt * taps[0:1, :] + cg * taps[1:2, :] + prv * taps[2:3, :]
    igg_v[...] = (value_grad * val_v[...].astype(F32)).astype(BF)
    vg_v[...] = (value_grad * ing_v[...].astype(F32)).astype(BF)
    store(8, igg_v, igg_out)
    store(9, vg_v, vg_out)

    await_bytes(rq_v.at[pl.ds(0, Z * Y - 1)], rq_recv.at[0])
    total = rq_v[0].astype(F32)
    for i in range(1, Z * Y):
        total = total + rq_v[i].astype(F32)
    proj_v[...] = total * (1.0 / math.sqrt(TOK * SP))
    store(10, proj_v, proj_out)

    ogopp.wait_send()
    for which, ref in ((0, out0_v), (1, out2_v)):
        await_bytes(ref.at[pl.ds(0, SLOTS - CAP), :], disp_sem.at[which])
        await_bytes(ref.at[pl.ds(0, SLOTS - CAP), :], ret_send.at[which])
    for copy in x_copies:
        copy.wait_send()
    for copy in p_copies.values():
        copy.wait_send()
    m2.wait_send()
    for copy in rf_copies:
        copy.wait_send()
    down.wait_send()
    up.wait_send()
    pair.wait_send()
    await_bytes(rq_v.at[pl.ds(0, Z * Y - 1)], rq_send.at[0])
    for copy in stores:
        copy.wait()


def grads_kernel(
    inp_ref, dgu_ref, hid_ref, routed_ref, resid_ref, ogg_ref, igg_ref, vg_ref, proj_ref,
    gate_out, up_out, down_out, resid_out, ogg_out, igg_out, vg_out, proj_out,
):
    scale = 1.0 / math.sqrt(SLOTS)
    both = mm(inp_ref[0], dgu_ref[...], (0, 0)) * scale
    gate_out[0] = both[:, :HID].astype(BF)
    up_out[0] = both[:, HID:].astype(BF)
    down_out[0] = (mm(hid_ref[...], routed_ref[0], (0, 0)) * scale).astype(BF)
    resid_out[...] = resid_ref[...]
    ogg_out[...] = ogg_ref[...]
    igg_out[...] = igg_ref[...]
    vg_out[...] = vg_ref[...]
    proj_out[...] = proj_ref[...]


def per_device(
    out_grad, route_ids, route_weight, expert_inputs, gate_weight, up_weight, down_weight,
    out_gate, in_gate, values, conv_out, conv_taps, proj_weight,
):
    sds = jax.ShapeDtypeStruct
    hbm = pl.BlockSpec(memory_space=pl.ANY)
    vm = pltpu.VMEM
    dma = pltpu.SemaphoreType.DMA
    act = (TOK, CH)
    outs = pl.pallas_call(
        layer_kernel,
        in_specs=[hbm] * 13,
        out_specs=[hbm] * 8,
        out_shape=[
            sds(act, BF), sds(act, BF), sds(act, BF), sds(act, BF), sds((ROWS, CH), F32),
            sds((TP, SLOTS, CH), BF), sds((SLOTS, HID), BF), sds((SLOTS, 2 * HID), BF),
        ],
        scratch_shapes=[
            vm((2, TOK), jnp.int32), vm((2, TOK), F32), vm(act, BF), vm((SLOTS, TP * CH), BF),
            vm((TP * CH, 2 * HID), BF), vm((HID, TP * CH), BF), vm(act, BF), vm(act, BF), vm(act, BF),
            vm(act, BF), vm((3, CH), BF), vm((TP * CH, CH), BF),
            vm(act, BF), vm((SLOTS, TOK), BF), vm((SLOTS, TOK), F32), vm((SLOTS, CH), BF),
            vm((SLOTS, CH), BF), vm((TP, SLOTS, CH), BF), vm((SLOTS, HID), F32), vm((SLOTS, HID), F32),
            vm((SLOTS, HID), BF), vm((SLOTS, 2 * HID), BF),
            vm((TP, SLOTS, CH), BF), vm((2, SLOTS, CH), BF), vm((SLOTS, CH), BF), vm((SLOTS, CH), BF),
            vm((SLOTS, CH), BF), vm(act, BF), vm(act, BF), vm((TP,) + act, BF), vm(act, BF), vm(act, BF),
            vm((16, CH), BF), vm((16, CH), BF),
            vm(act, BF), vm(act, BF), vm(act, BF), vm(act, BF), vm((Z * Y, C, ROWS, CH), BF),
            vm((Z * Y, ROWS, CH), BF), vm((Z * Y, ROWS, CH), BF), vm((Z * Y, ROWS, CH), BF),
            vm((ROWS, CH), F32),
            dma((13,)), dma((11,)), dma((2,)), dma((2,)), dma((Z,)), dma((Z,)), dma((2, Z)), dma((2, Z)),
            dma((2, Z)), dma((2, Z)), dma((2,)), dma((2,)), dma((2,)), dma((3,)), dma((3,)), dma((4,)),
            dma((2,)), dma((1,)), dma((1,)),
        ],
        compiler_params=pltpu.CompilerParams(
            collective_id=0, has_side_effects=True, vmem_limit_bytes=62 * 1024 * 1024
        ),
    )(
        route_ids.T, route_weight.T, out_grad, expert_inputs[0], gate_weight[0], up_weight[0],
        down_weight[0], out_gate, in_gate, values, conv_out, conv_taps, proj_weight,
    )
    resid, ogg, igg, vg, proj, routed, hid, dgu = outs
    steps = TP

    def whole(shape):
        return pl.BlockSpec(shape, lambda i: (0,) * len(shape))

    def strip(rows, cols=CH):
        return pl.BlockSpec((rows // steps, cols), lambda i: (i, 0))

    gate_grad, up_grad, down_grad, resid, ogg, igg, vg, proj = pl.pallas_call(
        grads_kernel,
        grid=(steps,),
        in_specs=[
            pl.BlockSpec((1, SLOTS, CH), lambda i: (0, 0, i)),
            whole((SLOTS, 2 * HID)),
            whole((SLOTS, HID)),
            pl.BlockSpec((1, SLOTS, CH), lambda i: (i, 0, 0)),
            strip(TOK), strip(TOK), strip(TOK), strip(TOK), strip(ROWS),
        ],
        out_specs=[
            pl.BlockSpec((1, CH, HID), lambda i: (0, i, 0)),
            pl.BlockSpec((1, CH, HID), lambda i: (0, i, 0)),
            pl.BlockSpec((1, HID, CH), lambda i: (0, 0, i)),
            strip(TOK), strip(TOK), strip(TOK), strip(TOK), strip(ROWS),
        ],
        out_shape=[
            sds((1, TP * CH, HID), BF), sds((1, TP * CH, HID), BF), sds((1, HID, TP * CH), BF),
            sds(act, BF), sds(act, BF), sds(act, BF), sds(act, BF), sds((ROWS, CH), F32),
        ],
        compiler_params=pltpu.CompilerParams(
            dimension_semantics=("arbitrary",), vmem_limit_bytes=48 * 1024 * 1024
        ),
    )(expert_inputs, dgu, hid, routed, resid, ogg, igg, vg, proj)
    return resid, ogg, igg, vg, proj, gate_grad, up_grad, down_grad


def solution(mesh):
    return jax.shard_map(
        per_device,
        mesh=mesh,
        in_specs=(
            P("sp", "tp"), P("sp", None), P("sp", None), P("sp", None, None), P("sp", None, "tp"),
            P("sp", None, "tp"), P("sp", "tp", None), P("sp", "tp"), P("sp", "tp"), P("sp", "tp"),
            P("sp", "tp"), P(None, "tp"), P(None, "tp"),
        ),
        out_specs=(
            P("sp", "tp"), P("sp", "tp"), P("sp", "tp"), P("sp", "tp"), P("sp", "tp"),
            P("sp", None, "tp"), P("sp", None, "tp"), P("sp", "tp", None),
        ),
        check_vma=False,
    )
```

```python
import functools
import math

import jax
import jax.numpy as jnp
from jax import lax
from jax.experimental import pallas as pl
from jax.experimental.pallas import tpu as pltpu
from jax.sharding import PartitionSpec as P

MESH = pl.DeviceIdType.MESH
BF = jnp.bfloat16
F32 = jnp.float32

Z, Y, C = 4, 4, 2
SP = Z * Y * C
TP = 4
TOK = 128
CAP = 16
SLOTS = SP * CAP
CH = 512
HID = 768
ROWS = 64
GROUP = Y * C
CHUNK = GROUP * CAP
ORDER = (0, 2, 1, 3)
FAR_FIRST = (2, 1, 3, 0)


def mm(a, b, dims):
    return lax.dot_general(a, b, ((dims[:1], dims[1:]), ((), ())), preferred_element_type=F32)


def at(block, size):
    return pl.ds(pl.multiple_of(block * size, size), size)


def layer_kernel(
    ids_hbm, w_hbm, og_hbm, inp_hbm, gw_hbm, uw_hbm, dw_hbm,
    gate_hbm, ing_hbm, val_hbm, conv_hbm, taps_hbm, pw_hbm,
    resid_v, ogg_v, igg_v, vg_v, proj_v, gate_grad_v, up_grad_v, down_grad_v,
    ids_v, w_v, og_v, inp_v, gu_v, dw_v, gate_v, ing_v, val_v, conv_v, taps_v, pw_v,
    ogopp_v, disp_v, wslot_v, out0_v, out2_v, r_v, s_v, a_v, hid_v, dgu_v,
    p_v, rp_v, b0_v, ret0_v, ret2_v, m2_v, r2_v, m0_v, rm0_v, rf_v, cg_v, before_v, after_v,
    zall_v, rft_v, rt_v,
    ld_sem, ogopp_sem, disp_sem, recv0_sem, recv2_sem, x_send, x_recv,
    pn_send, pn_recv, ret_send, ret_recv, m2_sem, m0_sem, rf_send, rf_recv, halo_sem, za_send, za_recv,
    zd_sem, rt_send, rt_recv,
):
    sp = lax.axis_index("sp")
    x = lax.axis_index("tp")
    z = sp // GROUP
    inner = lax.rem(sp, GROUP)
    core = lax.rem(sp, C)
    chip = sp // C
    y = lax.rem(chip, Y)
    xp, xm, xo = lax.rem(x + 1, TP), lax.rem(x + 3, TP), lax.rem(x + 2, TP)

    def load(i, src, dst):
        copy = pltpu.make_async_copy(src, dst, ld_sem.at[i])
        copy.start()
        return copy

    loads = [
        load(0, ids_hbm, ids_v),
        load(1, w_hbm, w_v),
        load(2, og_hbm, og_v),
        load(3, inp_hbm, inp_v),
        load(4, gw_hbm, gu_v.at[:, pl.ds(0, HID)]),
        load(5, uw_hbm, gu_v.at[:, pl.ds(HID, HID)]),
        load(6, dw_hbm, dw_v),
        load(7, gate_hbm, gate_v),
        load(8, conv_hbm, conv_v),
        load(9, pw_hbm, pw_v),
        load(10, ing_hbm, ing_v),
        load(11, val_hbm, val_v),
        load(12, taps_hbm, taps_v),
    ]

    barrier = pltpu.get_barrier_semaphore()

    def greet(i, carry):
        other = lax.rem(sp + 1 + i, SP)
        pl.semaphore_signal(barrier, inc=1, device_id=(other, x), device_id_type=MESH)
        return carry

    lax.fori_loop(0, SP - 1, greet, 0)
    for t in (xp, xm, xo):
        pl.semaphore_signal(barrier, inc=1, device_id=(sp, t), device_id_type=MESH)

    with jax.named_scope("w_load"):
        loads[0].wait()
        loads[1].wait()
        loads[2].wait()
    ids = ids_v[...]
    wts = w_v[...]
    e_iota = lax.broadcasted_iota(jnp.int32, (SP, TOK), 0)
    first = e_iota == ids[0:1, :]
    second = e_iota == ids[1:2, :]
    named = jnp.where(first | second, 1.0, 0.0)
    w_et = jnp.where(first, wts[0:1, :], 0.0) + jnp.where(second, wts[1:2, :], 0.0)
    earlier = lax.broadcasted_iota(jnp.int32, (TOK, TOK), 0) < lax.broadcasted_iota(
        jnp.int32, (TOK, TOK), 1
    )
    prefix = mm(named.astype(BF), jnp.where(earlier, 1.0, 0.0).astype(BF), (1, 0))
    rank = jnp.where(named > 0.5, prefix, -1.0)
    r_iota = lax.broadcasted_iota(jnp.int32, (SP, CAP, TOK), 1).astype(F32)
    hit = jnp.broadcast_to(rank[:, None, :], (SP, CAP, TOK)) == r_iota
    disp = jnp.where(hit, 1.0, 0.0)
    wslot = jnp.sum(disp * w_et[:, None, :], axis=2, keepdims=True)
    disp_v[...] = disp.reshape(SLOTS, TOK).astype(BF)
    wslot_v[...] = jnp.broadcast_to(wslot, (SP, CAP, TOK)).reshape(SLOTS, TOK)

    def dispatch(tok_ref, out_ref):
        rows = mm(disp_v[...], tok_ref[...], (1, 0))
        out_ref[...] = (rows * jnp.tile(wslot_v[...], (1, CH // TOK))).astype(BF)

    dispatch(og_v, out0_v)
    TILE = 256

    def hidden_tile(n):
        cols = slice(n * TILE, (n + 1) * TILE)
        ups = slice(HID + n * TILE, HID + (n + 1) * TILE)

        def rows_of(m, carry):
            rows = at(m, 256)
            pre_gate = mm(inp_v[rows, :], gu_v[:, cols], (1, 0))
            pre_up = mm(inp_v[rows, :], gu_v[:, ups], (1, 0))
            sig = 1.0 / (1.0 + jnp.exp(-pre_gate))
            act = pre_gate * sig
            s_v[rows, cols] = act
            a_v[rows, cols] = pre_up * sig * (1.0 + pre_gate * (1.0 - sig))
            hid_v[rows, cols] = (act * pre_up).astype(BF)
            return carry

        lax.fori_loop(0, SLOTS // 256, rows_of, 0)

    with jax.named_scope("w_weights"):
        loads[3].wait()
        loads[4].wait()
        loads[5].wait()
    hidden_tile(0)
    with jax.named_scope("w_barrier"):
        pl.semaphore_wait(barrier, SP - 1 + TP - 1)

    ogopp = pltpu.make_async_remote_copy(
        og_v, ogopp_v, ogopp_sem.at[0], ogopp_sem.at[1], device_id=(sp, xo), device_id_type=MESH
    )
    ogopp.start()

    def plane(zz, skip_self):
        peers = []
        for dy in FAR_FIRST:
            for dc in (1, 0):
                if not (skip_self and dy == 0 and dc == 0):
                    peers.append((zz * Y + lax.rem(y + dy, Y)) * C + lax.rem(core + dc, C))
        return peers

    def interleaved(dzs, sign):
        lists = [[(dz, there) for there in plane(lax.rem(z + sign * dz + Z, Z), dz == 0)] for dz in dzs]
        return [entry for i in range(GROUP) for entries in lists for entry in entries[i : i + 1]]

    def scatter(out_ref, block, which, recv_sem, dzs):
        if 0 in dzs:
            r_v[block, at(sp, CAP), :] = out_ref[at(sp, CAP), :]
        for dz, there in interleaved(dzs, -1):
            pltpu.make_async_remote_copy(
                out_ref.at[at(there, CAP), :],
                r_v.at[block, at(sp, CAP), :],
                disp_sem.at[which],
                recv_sem.at[dz],
                device_id=(there, x),
                device_id_type=MESH,
            ).start()

    def await_bytes(ref, sem):
        pltpu.make_async_copy(ref, ref, sem).wait()

    def chunk_rows(dz):
        return at(lax.rem(z + dz, Z), CHUNK)

    scatter(out0_v, 0, 0, recv0_sem, (2, 0))
    scatter(out0_v, 0, 0, recv0_sem, (1, 3))

    x_copies = []

    def await_group(block, dz, recv_sem):
        count = CHUNK - CAP if dz == 0 else CHUNK
        with jax.named_scope(f"w_group{block}_{dz}"):
            await_bytes(r_v.at[block, pl.ds(0, count), :], recv_sem.at[dz])

    def forward(k):
        dz = ORDER[k]
        await_group(0, dz, recv0_sem)
        for way, (there, landing) in enumerate(((xp, 3), (xm, 1))):
            copy = pltpu.make_async_remote_copy(
                r_v.at[0, chunk_rows(dz), :],
                r_v.at[landing, chunk_rows(dz), :],
                x_send.at[way, k],
                x_recv.at[way, k],
                device_id=(sp, there),
                device_id_type=MESH,
            )
            copy.start()
            x_copies.append(copy)

    loads[7].wait()
    loads[8].wait()
    gate_vals = gate_v[...].astype(F32)
    conv_vals = conv_v[...].astype(F32)
    zall_v[core, z, y] = (gate_vals * conv_vals).astype(BF)
    partner = sp + 1 - 2 * core
    zp, zm = lax.rem(z + 1, Z), lax.rem(z + 3, Z)
    yp, ym = lax.rem(y + 1, Y), lax.rem(y + 3, Y)
    west, east = pl.ds(0, CH // 2), pl.ds(CH // 2, CH // 2)
    low, high, full = pl.ds(0, TOK // 2), pl.ds(TOK // 2, TOK // 2), pl.ds(0, TOK)
    every = pl.ds(0, Z)
    z_copies = []

    def spread(phase):
        steps = (
            ((z, y, full, west), (z, y, full, west), (z, y, full, east), (z, y, full, east)),
            ((z, ym, low, west), (z, yp, high, west), (zm, y, low, east), (zp, y, high, east)),
            ((z, every, full, west), (z, every, full, west), (every, y, full, east), (every, y, full, east)),
            ((zm, every, low, west), (zp, every, high, west), (every, ym, low, east), (every, yp, high, east)),
        )[phase]
        along_y, along_z = ((z, yp), (z, ym)), ((zp, y), (zm, y))
        theres = along_y + along_z if phase < 2 else along_z + along_y
        if phase > 0:
            with jax.named_scope(f"w_spread{phase}"):
                for copy in z_copies[-4:]:
                    copy.wait_recv()
        for way, ((bz, by, rows, cols), (tz, ty)) in enumerate(zip(steps, theres)):
            part = zall_v.at[core, bz, by, rows, cols]
            copy = pltpu.make_async_remote_copy(
                part, part, za_send.at[phase, way], za_recv.at[phase, way],
                device_id=((tz * Y + ty) * C + core, x), device_id_type=MESH,
            )
            copy.start()
            z_copies.append(copy)

    spread(0)
    hidden_tile(1)
    forward(0)
    with jax.named_scope("w_ogopp"):
        ogopp.wait_recv()
    dispatch(ogopp_v, out2_v)
    scatter(out2_v, 2, 1, recv2_sem, (2, 0))
    forward(1)
    hidden_tile(2)
    spread(1)
    scatter(out2_v, 2, 1, recv2_sem, (1, 3))
    forward(2)
    forward(3)
    loads[6].wait()

    p_copies = {}

    def give_back(src_ref, dst_ref, which, dzs):
        if 0 in dzs:
            dst_ref[at(sp, CAP), :] = src_ref[at(sp, CAP), :]
        for _, there in interleaved(dzs, 1):
            pltpu.make_async_remote_copy(
                src_ref.at[at(there, CAP), :],
                dst_ref.at[at(sp, CAP), :],
                ret_send.at[which],
                ret_recv.at[which],
                device_id=(there, x),
                device_id_type=MESH,
            ).start()

    def finish_own(k):
        dz = ORDER[k]
        rows = chunk_rows(dz)
        with jax.named_scope(f"w_part{k}"):
            for way in range(2):
                p_copies[way, k].wait_recv()
        total = p_v[0, rows, :].astype(F32) + rp_v[0, rows, :].astype(F32) + rp_v[1, rows, :].astype(F32)
        b0_v[rows, :] = total.astype(BF)
        give_back(b0_v, ret0_v, 0, (dz,))

    def rows_pair(ref, halves):
        return jnp.concatenate([ref[rows, :] for rows in halves], axis=0)

    def put_pair(ref, halves, value):
        for h, rows in enumerate(halves):
            ref[rows, :] = value[h * CHUNK : (h + 1) * CHUNK, :]

    for ks in ((0, 1), (2, 3)):
        halves = [chunk_rows(ORDER[k]) for k in ks]
        for k in ks:
            await_group(2, ORDER[k], recv2_sem)
            with jax.named_scope(f"w_x{k}"):
                x_copies[2 * k].wait_recv()
                x_copies[2 * k + 1].wait_recv()
        d_hidden = None
        for j in range(TP):
            term = mm(rows_pair(r_v.at[j], halves), dw_v[:, at(lax.rem(x + j, TP), CH)], (1, 1))
            d_hidden = term if d_hidden is None else d_hidden + term
        if ks[0] == 0:
            spread(2)
        put_pair(dgu_v.at[:, pl.ds(0, HID)], halves, (d_hidden * rows_pair(a_v, halves)).astype(BF))
        put_pair(dgu_v.at[:, pl.ds(HID, HID)], halves, (d_hidden * rows_pair(s_v, halves)).astype(BF))
        for j in (1, 3, 2, 0):
            part = mm(rows_pair(dgu_v, halves), gu_v[at(lax.rem(x + j, TP), CH), :], (1, 1))
            put_pair(p_v.at[j], halves, part.astype(BF))
            if j in (1, 3):
                way = 0 if j == 1 else 1
                for k, rows in zip(ks, halves):
                    copy = pltpu.make_async_remote_copy(
                        p_v.at[j, rows, :],
                        rp_v.at[way, rows, :],
                        pn_send.at[way, k],
                        pn_recv.at[way, k],
                        device_id=(sp, xp if j == 1 else xm),
                        device_id_type=MESH,
                    )
                    copy.start()
                    p_copies[way, k] = copy
            if j == 2:
                give_back(p_v.at[2], ret2_v, 1, [ORDER[k] for k in ks])
                if ks[0] > 0:
                    spread(3)
        if ks[0] > 0:
            finish_own(0)
            finish_own(1)

    slot_scale = 1.0 / math.sqrt(SLOTS)

    def down_tiles(lower, upper):
        def tile(n, carry):
            rows = at(n, 256)
            turned = hid_v[:, rows].T
            for j in range(TP):
                part = mm(turned, r_v[j], (1, 0)) * slot_scale
                down_grad_v[rows, at(lax.rem(x + j, TP), CH)] = part.astype(BF)
            return carry

        lax.fori_loop(lower, upper, tile, 0)

    def gate_tiles(lower, upper):
        def tile(n, carry):
            rows = at(n, 256)
            turned = inp_v[:, rows].T
            gate_grad_v[rows, :] = (mm(turned, dgu_v[:, 0:HID], (1, 0)) * slot_scale).astype(BF)
            up_grad_v[rows, :] = (mm(turned, dgu_v[:, HID : 2 * HID], (1, 0)) * slot_scale).astype(BF)
            return carry

        lax.fori_loop(lower, upper, tile, 0)

    finish_own(2)
    finish_own(3)
    with jax.named_scope("g_gate"):
        gate_tiles(0, 4)
    with jax.named_scope("w_spread4"):
        for copy in z_copies[-4:]:
            copy.wait_recv()
    to_partner = pltpu.make_async_remote_copy(
        zall_v.at[core], zall_v.at[core], zd_sem.at[0], zd_sem.at[1],
        device_id=(partner, x), device_id_type=MESH,
    )
    to_partner.start()

    def await_returned(ref, which):
        with jax.named_scope(f"w_ret{which}"):
            await_bytes(ref.at[pl.ds(0, SLOTS - CAP), :], ret_recv.at[which])

    def to_opposite(src, dst, sem):
        copy = pltpu.make_async_remote_copy(
            src, dst, sem.at[0], sem.at[1], device_id=(sp, xo), device_id_type=MESH
        )
        copy.start()
        return copy

    await_returned(ret2_v, 1)
    m2_v[...] = mm(disp_v[...], ret2_v[...], (0, 0)).astype(BF)
    m2 = to_opposite(m2_v, r2_v, m2_sem)
    await_returned(ret0_v, 0)
    moe = mm(disp_v[...], ret0_v[...], (0, 0))
    m0_v[...] = moe.astype(BF)
    m0 = to_opposite(m0_v, rm0_v, m0_sem)
    with jax.named_scope("w_m2"):
        m2.wait_recv()
    own = (og_v[...].astype(F32) + moe + r2_v[...].astype(F32)).astype(BF)
    rf_v[0] = own
    rf_copies = []
    for i, (there, landing) in enumerate(((xp, 3), (xm, 1))):
        copy = pltpu.make_async_remote_copy(
            rf_v.at[0],
            rf_v.at[landing],
            rf_send.at[i],
            rf_recv.at[i],
            device_id=(sp, there),
            device_id_type=MESH,
        )
        copy.start()
        rf_copies.append(copy)
    resid_v[...] = own
    loads[9].wait()

    def mix_part(j):
        return mm(rf_v[j], pw_v[at(lax.rem(x + j, TP), CH), :], (1, 0))

    def order_of(cc, zz, yy):
        return (cc * Z + zz) * Y + yy

    mine = order_of(core, z, y)

    def share(j):
        block = lax.rem(x + j, TP)
        rft_v[j] = rf_v[j].T.reshape(GROUP, ROWS, TOK)

        for there in plane(block, False):
            inside = lax.rem(there, GROUP)

            @pl.when(there != sp)
            def _():
                pltpu.make_async_remote_copy(
                    rft_v.at[j, inside],
                    rt_v.at[mine],
                    rt_send.at[0],
                    rt_recv.at[lax.rem(z - block + Z, Z)],
                    device_id=(there, x),
                    device_id_type=MESH,
                ).start()

    share(0)
    mix = mix_part(0)
    with jax.named_scope("g_gate2"):
        gate_tiles(4, 8)
    for j, i in ((3, 0), (1, 1)):
        with jax.named_scope(f"w_rf{j}"):
            rf_copies[i].wait_recv()
        share(j)
        mix = mix + mix_part(j)
    with jax.named_scope("w_rf2"):
        m0.wait_recv()
    rf_v[2] = (ogopp_v[...].astype(F32) + rm0_v[...].astype(F32) + m2_v[...].astype(F32)).astype(BF)
    mix = mix + mix_part(2)
    ogg_v[...] = (mix * conv_vals).astype(BF)
    cg_v[...] = (mix * gate_vals).astype(BF)
    down = pltpu.make_async_remote_copy(
        cg_v.at[pl.ds(0, 16), :], after_v, halo_sem.at[0], halo_sem.at[1],
        device_id=(lax.rem(sp + SP - 1, SP), x), device_id_type=MESH,
    )
    up = pltpu.make_async_remote_copy(
        cg_v.at[pl.ds(TOK - 16, 16), :], before_v, halo_sem.at[2], halo_sem.at[3],
        device_id=(lax.rem(sp + 1, SP), x), device_id_type=MESH,
    )
    down.start()
    up.start()
    share(2)
    rt_v[mine] = rft_v[lax.rem(z - x + TP, TP), inner]
    with jax.named_scope("g_down"):
        down_tiles(0, HID // 256)
    with jax.named_scope("w_zd"):
        to_partner.wait_recv()

    def proj_group(dz):
        count = GROUP - 1 if dz == 0 else GROUP
        with jax.named_scope(f"w_rt{dz}"):
            await_bytes(rt_v.at[pl.ds(0, count)], rt_recv.at[dz])
        zz = lax.rem(z + dz, Z)
        total = None
        for cc in range(C):
            left = jnp.concatenate([rt_v[order_of(cc, zz, yy)] for yy in range(Y)], axis=1)
            term = mm(left, zall_v[cc, zz].reshape(Y * TOK, CH), (1, 0))
            total = term if total is None else total + term
        return total

    proj = proj_group(0) + proj_group(1)

    loads[10].wait()
    loads[11].wait()
    loads[12].wait()
    with jax.named_scope("w_halo"):
        down.wait_recv()
        up.wait_recv()
    cg = cg_v[...].astype(F32)
    taps = taps_v[...].astype(F32)
    row = lax.broadcasted_iota(jnp.int32, (TOK, CH), 0)
    has_before = jnp.where(sp > 0, 1.0, 0.0)
    has_after = jnp.where(sp < SP - 1, 1.0, 0.0)
    before = before_v[...].astype(F32)[15:16, :] * has_before
    after = after_v[...].astype(F32)[0:1, :] * has_after
    nxt = jnp.where(row == TOK - 1, jnp.broadcast_to(after, (TOK, CH)), pltpu.roll(cg, TOK - 1, 0))
    prv = jnp.where(row == 0, jnp.broadcast_to(before, (TOK, CH)), pltpu.roll(cg, 1, 0))
    value_grad = nxt * taps[0:1, :] + cg * taps[1:2, :] + prv * taps[2:3, :]
    igg_v[...] = (value_grad * val_v[...].astype(F32)).astype(BF)
    vg_v[...] = (value_grad * ing_v[...].astype(F32)).astype(BF)

    proj = proj + proj_group(3)
    proj = proj + proj_group(2)
    proj_v[...] = proj * (1.0 / math.sqrt(TOK * SP))

    ogopp.wait_send()
    for which, ref in ((0, out0_v), (1, out2_v)):
        await_bytes(ref.at[pl.ds(0, SLOTS - CAP), :], disp_sem.at[which])
        await_bytes(ref.at[pl.ds(0, SLOTS - CAP), :], ret_send.at[which])
    for copy in x_copies:
        copy.wait_send()
    for copy in p_copies.values():
        copy.wait_send()
    m2.wait_send()
    for copy in rf_copies:
        copy.wait_send()
    down.wait_send()
    up.wait_send()
    m0.wait_send()
    to_partner.wait_send()
    for copy in z_copies:
        copy.wait_send()
    await_bytes(rt_v.at[pl.ds(0, SP - 1)], rt_send.at[0])


def flush_kernel(*refs):
    count = (len(refs) - 1) // 2
    sems = refs[-1]
    copies = []
    for i in range(count):
        src, dst = refs[i], refs[count + i]
        pieces = 4 if i >= count - 3 else 1
        rows = src.shape[0] // pieces
        for p in range(pieces):
            part = pl.ds(p * rows, rows)
            copies.append(pltpu.make_async_copy(src.at[part, :], dst.at[part, :], sems.at[i, p]))
    for copy in copies:
        copy.start()
    for copy in copies:
        copy.wait()


def per_device(
    out_grad, route_ids, route_weight, expert_inputs, gate_weight, up_weight, down_weight,
    out_gate, in_gate, values, conv_out, conv_taps, proj_weight,
):
    sds = jax.ShapeDtypeStruct
    hbm = pl.BlockSpec(memory_space=pltpu.HBM)
    vm = pltpu.VMEM
    dma = pltpu.SemaphoreType.DMA
    act = (TOK, CH)
    vmem = pl.BlockSpec(memory_space=pltpu.VMEM)
    shapes = [
        sds(act, BF), sds(act, BF), sds(act, BF), sds(act, BF), sds((ROWS, CH), F32),
        sds((TP * CH, HID), BF), sds((TP * CH, HID), BF), sds((HID, TP * CH), BF),
    ]
    outs = pl.pallas_call(
        layer_kernel,
        in_specs=[hbm] * 13,
        out_specs=[vmem] * 8,
        out_shape=[vm(o.shape, o.dtype) for o in shapes],
        scratch_shapes=[
            vm((2, TOK), jnp.int32), vm((2, TOK), F32), vm(act, BF), vm((SLOTS, TP * CH), BF),
            vm((TP * CH, 2 * HID), BF), vm((HID, TP * CH), BF), vm(act, BF), vm(act, BF), vm(act, BF),
            vm(act, BF), vm((3, CH), BF), vm((TP * CH, CH), BF),
            vm(act, BF), vm((SLOTS, TOK), BF), vm((SLOTS, TOK), F32), vm((SLOTS, CH), BF),
            vm((SLOTS, CH), BF), vm((TP, SLOTS, CH), BF), vm((SLOTS, HID), F32), vm((SLOTS, HID), F32),
            vm((SLOTS, HID), BF), vm((SLOTS, 2 * HID), BF),
            vm((TP, SLOTS, CH), BF), vm((2, SLOTS, CH), BF), vm((SLOTS, CH), BF), vm((SLOTS, CH), BF),
            vm((SLOTS, CH), BF), vm(act, BF), vm(act, BF), vm(act, BF), vm(act, BF),
            vm((TP,) + act, BF), vm(act, BF), vm((16, CH), BF), vm((16, CH), BF),
            vm((C, Z, Y) + act, BF), vm((TP, GROUP, ROWS, TOK), BF), vm((SP, ROWS, TOK), BF),
            dma((13,)), dma((2,)), dma((2,)), dma((Z,)), dma((Z,)), dma((2, Z)), dma((2, Z)),
            dma((2, Z)), dma((2, Z)), dma((2,)), dma((2,)), dma((2,)), dma((2,)), dma((2,)), dma((2,)),
            dma((4,)), dma((4, 4)), dma((4, 4)), dma((2,)), dma((1,)), dma((Z,)),
        ],
        compiler_params=pltpu.CompilerParams(
            collective_id=0, has_side_effects=True, vmem_limit_bytes=52428800
        ),
    )(
        route_ids.T, route_weight.T, out_grad, expert_inputs[0], gate_weight[0], up_weight[0],
        down_weight[0], out_gate, in_gate, values, conv_out, conv_taps, proj_weight,
    )
    resid, ogg, igg, vg, proj, gate_grad, up_grad, down_grad = pl.pallas_call(
        flush_kernel,
        in_specs=[vmem] * 8,
        out_specs=[hbm] * 8,
        out_shape=shapes,
        scratch_shapes=[dma((8, 4))],
        compiler_params=pltpu.CompilerParams(vmem_limit_bytes=1024 * 1024),
    )(*outs)
    return resid, ogg, igg, vg, proj, gate_grad[None], up_grad[None], down_grad[None]


def solution(mesh):
    return jax.shard_map(
        per_device,
        mesh=mesh,
        in_specs=(
            P("sp", "tp"), P("sp", None), P("sp", None), P("sp", None, None), P("sp", None, "tp"),
            P("sp", None, "tp"), P("sp", "tp", None), P("sp", "tp"), P("sp", "tp"), P("sp", "tp"),
            P("sp", "tp"), P(None, "tp"), P(None, "tp"),
        ),
        out_specs=(
            P("sp", "tp"), P("sp", "tp"), P("sp", "tp"), P("sp", "tp"), P("sp", "tp"),
            P("sp", None, "tp"), P("sp", None, "tp"), P("sp", "tp", None),
        ),
        check_vma=False,
    )
```

```python
import functools
import math

import jax
import jax.numpy as jnp
from jax import lax
from jax.experimental import pallas as pl
from jax.experimental.pallas import tpu as pltpu
from jax.sharding import PartitionSpec as P

MESH = pl.DeviceIdType.MESH
BF = jnp.bfloat16
F32 = jnp.float32

Z, Y, C = 4, 4, 2
SP = Z * Y * C
TP = 4
TOK = 128
CAP = 16
SLOTS = SP * CAP
CH = 512
HID = 768
ROWS = 64
GROUP = Y * C
CHUNK = GROUP * CAP
ORDER = (0, 2, 1, 3)
FAR_FIRST = (2, 1, 3, 0)


def mm(a, b, dims):
    return lax.dot_general(a, b, ((dims[:1], dims[1:]), ((), ())), preferred_element_type=F32)


def at(block, size):
    return pl.ds(pl.multiple_of(block * size, size), size)


def layer_kernel(
    ids_hbm, w_hbm, og_hbm, inp_hbm, gw_hbm, uw_hbm, dw_hbm,
    gate_hbm, ing_hbm, val_hbm, conv_hbm, taps_hbm, pw_hbm,
    resid_v, ogg_v, igg_v, vg_v, proj_v, gate_grad_v, up_grad_v, down_grad_v,
    ids_v, w_v, og_v, inp_v, gu_v, dw_v, gate_v, ing_v, val_v, conv_v, taps_v, pw_v,
    ogopp_v, disp_v, wslot_v, out0_v, out2_v, r_v, s_v, a_v, hid_v, dgu_v,
    p_v, rp_v, b0_v, ret0_v, ret2_v, m2_v, r2_v, m0_v, rm0_v, rf_v, cg_v, before_v, after_v,
    zall_v, rft_v, rt_v,
    ld_sem, ogopp_sem, disp_sem, recv0_sem, recv2_sem, x_send, x_recv,
    pn_send, pn_recv, ret_send, ret_recv, m2_sem, m0_sem, rf_send, rf_recv, halo_sem, za_send, za_recv,
    zd_sem, rt_send, rt_recv,
):
    sp = lax.axis_index("sp")
    x = lax.axis_index("tp")
    z = sp // GROUP
    inner = lax.rem(sp, GROUP)
    core = lax.rem(sp, C)
    chip = sp // C
    y = lax.rem(chip, Y)
    xp, xm, xo = lax.rem(x + 1, TP), lax.rem(x + 3, TP), lax.rem(x + 2, TP)

    def load(i, src, dst):
        copy = pltpu.make_async_copy(src, dst, ld_sem.at[i])
        copy.start()
        return copy

    def blocks(i, pairs):
        for j in range(TP):
            for src, dst in pairs(at(lax.rem(x + j, TP), CH), pl.ds(j * CH, CH)):
                load(i, src, dst)

    loads = {
        0: load(0, ids_hbm, ids_v),
        1: load(1, w_hbm, w_v),
        2: load(2, og_hbm, og_v),
        7: load(7, gate_hbm, gate_v),
        8: load(8, conv_hbm, conv_v),
    }
    blocks(3, lambda theirs, ours: [(inp_hbm.at[:, theirs], inp_v.at[:, ours])])
    blocks(4, lambda theirs, ours: [
        (gw_hbm.at[theirs, :], gu_v.at[ours, pl.ds(0, HID)]),
        (uw_hbm.at[theirs, :], gu_v.at[ours, pl.ds(HID, HID)]),
    ])
    blocks(6, lambda theirs, ours: [(dw_hbm.at[:, theirs], dw_v.at[:, ours])])
    loads |= {
        9: load(9, pw_hbm, pw_v),
        10: load(10, ing_hbm, ing_v),
        11: load(11, val_hbm, val_v),
        12: load(12, taps_hbm, taps_v),
    }

    def await_bytes(ref, sem):
        pltpu.make_async_copy(ref, ref, sem).wait()


    barrier = pltpu.get_barrier_semaphore()

    def greet(i, carry):
        other = lax.rem(sp + 1 + i, SP)
        pl.semaphore_signal(barrier, inc=1, device_id=(other, x), device_id_type=MESH)
        return carry

    lax.fori_loop(0, SP - 1, greet, 0)
    for t in (xp, xm, xo):
        pl.semaphore_signal(barrier, inc=1, device_id=(sp, t), device_id_type=MESH)

    with jax.named_scope("w_load"):
        loads[0].wait()
        loads[1].wait()
        loads[2].wait()
    ids = ids_v[...]
    wts = w_v[...]
    e_iota = lax.broadcasted_iota(jnp.int32, (SP, TOK), 0)
    first = e_iota == ids[0:1, :]
    second = e_iota == ids[1:2, :]
    named = jnp.where(first | second, 1.0, 0.0)
    w_et = jnp.where(first, wts[0:1, :], 0.0) + jnp.where(second, wts[1:2, :], 0.0)
    earlier = lax.broadcasted_iota(jnp.int32, (TOK, TOK), 0) < lax.broadcasted_iota(
        jnp.int32, (TOK, TOK), 1
    )
    prefix = mm(named.astype(BF), jnp.where(earlier, 1.0, 0.0).astype(BF), (1, 0))
    rank = jnp.where(named > 0.5, prefix, -1.0)
    r_iota = lax.broadcasted_iota(jnp.int32, (SP, CAP, TOK), 1).astype(F32)
    hit = jnp.broadcast_to(rank[:, None, :], (SP, CAP, TOK)) == r_iota
    disp = jnp.where(hit, 1.0, 0.0)
    wslot = jnp.sum(disp * w_et[:, None, :], axis=2, keepdims=True)
    disp_v[...] = disp.reshape(SLOTS, TOK).astype(BF)
    wslot_v[...] = jnp.broadcast_to(wslot, (SP, CAP, TOK)).reshape(SLOTS, TOK)

    def dispatch(tok_ref, out_ref):
        rows = mm(disp_v[...], tok_ref[...], (1, 0))
        out_ref[...] = (rows * jnp.tile(wslot_v[...], (1, CH // TOK))).astype(BF)

    dispatch(og_v, out0_v)
    TILE = 256

    def hidden_tile(n):
        cols = slice(n * TILE, (n + 1) * TILE)
        ups = slice(HID + n * TILE, HID + (n + 1) * TILE)

        def rows_of(m, carry):
            rows = at(m, 256)
            pre_gate = mm(inp_v[rows, :], gu_v[:, cols], (1, 0))
            pre_up = mm(inp_v[rows, :], gu_v[:, ups], (1, 0))
            sig = 1.0 / (1.0 + jnp.exp(-pre_gate))
            act = pre_gate * sig
            s_v[rows, cols] = act
            a_v[rows, cols] = pre_up * sig * (1.0 + pre_gate * (1.0 - sig))
            hid_v[rows, cols] = (act * pre_up).astype(BF)
            return carry

        lax.fori_loop(0, SLOTS // 256, rows_of, 0)

    with jax.named_scope("w_barrier"):
        pl.semaphore_wait(barrier, SP - 1 + TP - 1)

    ogopp = pltpu.make_async_remote_copy(
        og_v, ogopp_v, ogopp_sem.at[0], ogopp_sem.at[1], device_id=(sp, xo), device_id_type=MESH
    )
    ogopp.start()

    def plane(zz, skip_self):
        peers = []
        for dy in FAR_FIRST:
            for dc in (1, 0):
                if not (skip_self and dy == 0 and dc == 0):
                    peers.append((zz * Y + lax.rem(y + dy, Y)) * C + lax.rem(core + dc, C))
        return peers

    def interleaved(dzs, sign):
        lists = [[(dz, there) for there in plane(lax.rem(z + sign * dz + Z, Z), dz == 0)] for dz in dzs]
        return [entry for i in range(GROUP) for entries in lists for entry in entries[i : i + 1]]

    def scatter(out_ref, block, which, recv_sem, dzs):
        if 0 in dzs:
            r_v[block, at(sp, CAP), :] = out_ref[at(sp, CAP), :]
        for dz, there in interleaved(dzs, -1):
            pltpu.make_async_remote_copy(
                out_ref.at[at(there, CAP), :],
                r_v.at[block, at(sp, CAP), :],
                disp_sem.at[which],
                recv_sem.at[dz],
                device_id=(there, x),
                device_id_type=MESH,
            ).start()

    def chunk_rows(dz):
        return at(lax.rem(z + dz, Z), CHUNK)

    scatter(out0_v, 0, 0, recv0_sem, (0,))
    scatter(out0_v, 0, 0, recv0_sem, (2,))
    scatter(out0_v, 0, 0, recv0_sem, (1, 3))

    x_copies = []

    def await_group(block, dz, recv_sem):
        count = CHUNK - CAP if dz == 0 else CHUNK
        with jax.named_scope(f"w_group{block}_{dz}"):
            await_bytes(r_v.at[block, pl.ds(0, count), :], recv_sem.at[dz])

    def forward(k):
        dz = ORDER[k]
        await_group(0, dz, recv0_sem)
        for way, (there, landing) in enumerate(((xp, 3), (xm, 1))):
            copy = pltpu.make_async_remote_copy(
                r_v.at[0, chunk_rows(dz), :],
                r_v.at[landing, chunk_rows(dz), :],
                x_send.at[way, k],
                x_recv.at[way, k],
                device_id=(sp, there),
                device_id_type=MESH,
            )
            copy.start()
            x_copies.append(copy)

    loads[7].wait()
    loads[8].wait()
    gate_vals = gate_v[...].astype(F32)
    conv_vals = conv_v[...].astype(F32)
    zall_v[core, z, y] = (gate_vals * conv_vals).astype(BF)
    partner = sp + 1 - 2 * core
    zp, zm = lax.rem(z + 1, Z), lax.rem(z + 3, Z)
    yp, ym = lax.rem(y + 1, Y), lax.rem(y + 3, Y)
    west, east = pl.ds(0, CH // 2), pl.ds(CH // 2, CH // 2)
    low, high, full = pl.ds(0, TOK // 2), pl.ds(TOK // 2, TOK // 2), pl.ds(0, TOK)
    every = pl.ds(0, Z)
    z_copies = []

    def spread(phase):
        steps = (
            ((z, y, full, west), (z, y, full, west), (z, y, full, east), (z, y, full, east)),
            ((z, ym, low, west), (z, yp, high, west), (zm, y, low, east), (zp, y, high, east)),
            ((z, every, full, west), (z, every, full, west), (every, y, full, east), (every, y, full, east)),
            ((zm, every, low, west), (zp, every, high, west), (every, ym, low, east), (every, yp, high, east)),
        )[phase]
        along_y, along_z = ((z, yp), (z, ym)), ((zp, y), (zm, y))
        theres = along_y + along_z if phase < 2 else along_z + along_y
        if phase > 0:
            with jax.named_scope(f"w_spread{phase}"):
                for copy in z_copies[-4:]:
                    copy.wait_recv()
        for way, ((bz, by, rows, cols), (tz, ty)) in enumerate(zip(steps, theres)):
            part = zall_v.at[core, bz, by, rows, cols]
            copy = pltpu.make_async_remote_copy(
                part, part, za_send.at[phase, way], za_recv.at[phase, way],
                device_id=((tz * Y + ty) * C + core, x), device_id_type=MESH,
            )
            copy.start()
            z_copies.append(copy)

    spread(0)
    with jax.named_scope("w_weights"):
        await_bytes(inp_v, ld_sem.at[3])
        await_bytes(gu_v, ld_sem.at[4])
    hidden_tile(0)
    hidden_tile(1)
    forward(0)
    with jax.named_scope("w_ogopp"):
        ogopp.wait_recv()
    dispatch(ogopp_v, out2_v)
    scatter(out2_v, 2, 1, recv2_sem, (2, 0))
    forward(1)
    hidden_tile(2)
    spread(1)
    scatter(out2_v, 2, 1, recv2_sem, (1, 3))
    forward(2)
    forward(3)
    await_bytes(dw_v, ld_sem.at[6])

    p_copies = {}

    def give_back(src_ref, dst_ref, which, dzs):
        if 0 in dzs:
            dst_ref[at(sp, CAP), :] = src_ref[at(sp, CAP), :]
        for _, there in interleaved(dzs, 1):
            pltpu.make_async_remote_copy(
                src_ref.at[at(there, CAP), :],
                dst_ref.at[at(sp, CAP), :],
                ret_send.at[which],
                ret_recv.at[which],
                device_id=(there, x),
                device_id_type=MESH,
            ).start()

    def finish_own(k):
        dz = ORDER[k]
        rows = chunk_rows(dz)
        with jax.named_scope(f"w_part{k}"):
            for way in range(2):
                p_copies[way, k].wait_recv()
        total = p_v[0, rows, :].astype(F32) + rp_v[0, rows, :].astype(F32) + rp_v[1, rows, :].astype(F32)
        b0_v[rows, :] = total.astype(BF)
        give_back(b0_v, ret0_v, 0, (dz,))

    def rows_pair(ref, halves):
        return jnp.concatenate([ref[rows, :] for rows in halves], axis=0)

    def put_pair(ref, halves, value):
        for h, rows in enumerate(halves):
            ref[rows, :] = value[h * CHUNK : (h + 1) * CHUNK, :]

    for ks in ((0, 1), (2, 3)):
        halves = [chunk_rows(ORDER[k]) for k in ks]
        for k in ks:
            await_group(2, ORDER[k], recv2_sem)
            with jax.named_scope(f"w_x{k}"):
                x_copies[2 * k].wait_recv()
                x_copies[2 * k + 1].wait_recv()
        left = jnp.concatenate([rows_pair(r_v.at[j], halves) for j in range(TP)], axis=1)
        d_hidden = mm(left, dw_v[...], (1, 1))
        if ks[0] == 0:
            spread(2)
        put_pair(dgu_v.at[:, pl.ds(0, HID)], halves, (d_hidden * rows_pair(a_v, halves)).astype(BF))
        put_pair(dgu_v.at[:, pl.ds(HID, HID)], halves, (d_hidden * rows_pair(s_v, halves)).astype(BF))
        for j in (1, 3, 2, 0):
            part = mm(rows_pair(dgu_v, halves), gu_v[j * CH : (j + 1) * CH, :], (1, 1))
            put_pair(p_v.at[j], halves, part.astype(BF))
            if j in (1, 3):
                way = 0 if j == 1 else 1
                for k, rows in zip(ks, halves):
                    copy = pltpu.make_async_remote_copy(
                        p_v.at[j, rows, :],
                        rp_v.at[way, rows, :],
                        pn_send.at[way, k],
                        pn_recv.at[way, k],
                        device_id=(sp, xp if j == 1 else xm),
                        device_id_type=MESH,
                    )
                    copy.start()
                    p_copies[way, k] = copy
            if j == 2:
                give_back(p_v.at[2], ret2_v, 1, [ORDER[k] for k in ks])
    finish_own(0)
    finish_own(1)

    slot_scale = 1.0 / math.sqrt(SLOTS)

    def down_tiles(lower, upper):
        def tile(n, carry):
            rows = at(n, 256)
            turned = hid_v[:, rows].T
            for j in range(TP):
                part = mm(turned, r_v[j], (1, 0)) * slot_scale
                down_grad_v[rows, at(lax.rem(x + j, TP), CH)] = part.astype(BF)
            return carry

        lax.fori_loop(lower, upper, tile, 0)

    def gate_tiles(lower, upper):
        def tile(n, carry):
            rows = at(n, 256)
            turned = inp_v[:, rows].T
            rows = at(lax.rem(x + n // 2, TP) * 2 + lax.rem(n, 2), 256)
            gate_grad_v[rows, :] = (mm(turned, dgu_v[:, 0:HID], (1, 0)) * slot_scale).astype(BF)
            up_grad_v[rows, :] = (mm(turned, dgu_v[:, HID : 2 * HID], (1, 0)) * slot_scale).astype(BF)
            return carry

        lax.fori_loop(lower, upper, tile, 0)

    finish_own(2)
    finish_own(3)
    spread(3)

    def await_returned(ref, which):
        with jax.named_scope(f"w_ret{which}"):
            await_bytes(ref.at[pl.ds(0, SLOTS - CAP), :], ret_recv.at[which])

    def to_opposite(src, dst, sem):
        copy = pltpu.make_async_remote_copy(
            src, dst, sem.at[0], sem.at[1], device_id=(sp, xo), device_id_type=MESH
        )
        copy.start()
        return copy

    await_returned(ret2_v, 1)
    m2_v[...] = mm(disp_v[...], ret2_v[...], (0, 0)).astype(BF)
    m2 = to_opposite(m2_v, r2_v, m2_sem)
    with jax.named_scope("g_gate"):
        gate_tiles(0, 4)
    await_returned(ret0_v, 0)
    moe = mm(disp_v[...], ret0_v[...], (0, 0))
    m0_v[...] = moe.astype(BF)
    sides = (west, east)
    m0 = [to_opposite(m0_v.at[:, cols], rm0_v.at[:, cols], m0_sem.at[h]) for h, cols in enumerate(sides)]
    with jax.named_scope("w_m2"):
        m2.wait_recv()
    own = (og_v[...].astype(F32) + moe + r2_v[...].astype(F32)).astype(BF)
    rf_v[0] = own
    rf_copies = {}
    for h, cols in enumerate(sides):
        for there, landing in ((xp, 3), (xm, 1)):
            copy = pltpu.make_async_remote_copy(
                rf_v.at[0, :, cols],
                rf_v.at[landing, :, cols],
                rf_send.at[landing // 2, h],
                rf_recv.at[landing // 2, h],
                device_id=(sp, there),
                device_id_type=MESH,
            )
            copy.start()
            rf_copies[landing, h] = copy
    resid_v[...] = own
    loads[9].wait()

    def mix_part(j):
        return mm(rf_v[j], pw_v[at(lax.rem(x + j, TP), CH), :], (1, 0))

    def order_of(cc, zz, yy):
        return (cc * Z + zz) * Y + yy

    mine = order_of(core, z, y)

    HALF = GROUP // 2

    def share(j, h):
        block = lax.rem(x + j, TP)
        turned = rf_v[j, :, h * CH // 2 : (h + 1) * CH // 2].T
        rft_v[j, h * HALF : (h + 1) * HALF] = turned.reshape(HALF, ROWS, TOK)
        for dy in (1, 0):
            for dc in (1, 0):
                inside = (2 * h + lax.rem(y + dy, 2)) * C + lax.rem(core + dc, C)
                there = block * GROUP + inside

                @pl.when(there != sp)
                def _():
                    pltpu.make_async_remote_copy(
                        rft_v.at[j, inside],
                        rt_v.at[mine],
                        rt_send.at[0],
                        rt_recv.at[lax.rem(z - block + Z, Z)],
                        device_id=(there, x),
                        device_id_type=MESH,
                    ).start()

    share(0, 0)
    share(0, 1)
    mix = mix_part(0)
    with jax.named_scope("g_gate2"):
        gate_tiles(4, 8)
    with jax.named_scope("w_spread4"):
        for copy in z_copies[-4:]:
            copy.wait_recv()
    to_partner = pltpu.make_async_remote_copy(
        zall_v.at[core], zall_v.at[core], zd_sem.at[0], zd_sem.at[1],
        device_id=(partner, x), device_id_type=MESH,
    )
    to_partner.start()
    for h, cols in enumerate(sides):
        for j in (3, 1):
            with jax.named_scope(f"w_rf{j}_{h}"):
                rf_copies[j, h].wait_recv()
            share(j, h)
        with jax.named_scope(f"w_rf2_{h}"):
            m0[h].wait_recv()
        other = ogopp_v[:, cols].astype(F32) + rm0_v[:, cols].astype(F32) + m2_v[:, cols].astype(F32)
        rf_v[2, :, cols] = other.astype(BF)
        if h == 0:
            share(2, 0)
    for j in (3, 1, 2):
        mix = mix + mix_part(j)
    ogg_v[...] = (mix * conv_vals).astype(BF)
    cg_v[...] = (mix * gate_vals).astype(BF)
    down = pltpu.make_async_remote_copy(
        cg_v.at[pl.ds(0, 16), :], after_v, halo_sem.at[0], halo_sem.at[1],
        device_id=(lax.rem(sp + SP - 1, SP), x), device_id_type=MESH,
    )
    up = pltpu.make_async_remote_copy(
        cg_v.at[pl.ds(TOK - 16, 16), :], before_v, halo_sem.at[2], halo_sem.at[3],
        device_id=(lax.rem(sp + 1, SP), x), device_id_type=MESH,
    )
    down.start()
    up.start()
    share(2, 1)
    rt_v[mine] = rft_v[lax.rem(z - x + TP, TP), inner]
    with jax.named_scope("g_down"):
        down_tiles(0, HID // 256)
    with jax.named_scope("w_zd"):
        to_partner.wait_recv()

    def proj_group(dz):
        count = GROUP - 1 if dz == 0 else GROUP
        with jax.named_scope(f"w_rt{dz}"):
            await_bytes(rt_v.at[pl.ds(0, count)], rt_recv.at[dz])
        zz = lax.rem(z + dz, Z)
        total = None
        for cc in range(C):
            left = jnp.concatenate([rt_v[order_of(cc, zz, yy)] for yy in range(Y)], axis=1)
            term = mm(left, zall_v[cc, zz].reshape(Y * TOK, CH), (1, 0))
            total = term if total is None else total + term
        return total

    proj = proj_group(0) + proj_group(1)

    loads[10].wait()
    loads[11].wait()
    loads[12].wait()
    with jax.named_scope("w_halo"):
        down.wait_recv()
        up.wait_recv()
    cg = cg_v[...].astype(F32)
    taps = taps_v[...].astype(F32)
    row = lax.broadcasted_iota(jnp.int32, (TOK, CH), 0)
    has_before = jnp.where(sp > 0, 1.0, 0.0)
    has_after = jnp.where(sp < SP - 1, 1.0, 0.0)
    before = before_v[...].astype(F32)[15:16, :] * has_before
    after = after_v[...].astype(F32)[0:1, :] * has_after
    nxt = jnp.where(row == TOK - 1, jnp.broadcast_to(after, (TOK, CH)), pltpu.roll(cg, TOK - 1, 0))
    prv = jnp.where(row == 0, jnp.broadcast_to(before, (TOK, CH)), pltpu.roll(cg, 1, 0))
    value_grad = nxt * taps[0:1, :] + cg * taps[1:2, :] + prv * taps[2:3, :]
    igg_v[...] = (value_grad * val_v[...].astype(F32)).astype(BF)
    vg_v[...] = (value_grad * ing_v[...].astype(F32)).astype(BF)

    proj = proj + proj_group(3)
    proj = proj + proj_group(2)
    proj_v[...] = proj * (1.0 / math.sqrt(TOK * SP))

    ogopp.wait_send()
    for which, ref in ((0, out0_v), (1, out2_v)):
        await_bytes(ref.at[pl.ds(0, SLOTS - CAP), :], disp_sem.at[which])
        await_bytes(ref.at[pl.ds(0, SLOTS - CAP), :], ret_send.at[which])
    for copy in x_copies:
        copy.wait_send()
    for copy in p_copies.values():
        copy.wait_send()
    m2.wait_send()
    for copy in rf_copies.values():
        copy.wait_send()
    down.wait_send()
    up.wait_send()
    for copy in m0:
        copy.wait_send()
    to_partner.wait_send()
    for copy in z_copies:
        copy.wait_send()
    await_bytes(rt_v.at[pl.ds(0, SP - 1)], rt_send.at[0])


def flush_kernel(*refs):
    count = (len(refs) - 1) // 2
    sems = refs[-1]
    copies = []
    for i in range(count):
        src, dst = refs[i], refs[count + i]
        pieces = 4 if i >= count - 3 else 1
        rows = src.shape[0] // pieces
        for p in range(pieces):
            part = pl.ds(p * rows, rows)
            copies.append(pltpu.make_async_copy(src.at[part, :], dst.at[part, :], sems.at[i, p]))
    for copy in copies:
        copy.start()
    for copy in copies:
        copy.wait()


def per_device(
    out_grad, route_ids, route_weight, expert_inputs, gate_weight, up_weight, down_weight,
    out_gate, in_gate, values, conv_out, conv_taps, proj_weight,
):
    sds = jax.ShapeDtypeStruct
    hbm = pl.BlockSpec(memory_space=pltpu.HBM)
    vm = pltpu.VMEM
    dma = pltpu.SemaphoreType.DMA
    act = (TOK, CH)
    vmem = pl.BlockSpec(memory_space=pltpu.VMEM)
    shapes = [
        sds(act, BF), sds(act, BF), sds(act, BF), sds(act, BF), sds((ROWS, CH), F32),
        sds((TP * CH, HID), BF), sds((TP * CH, HID), BF), sds((HID, TP * CH), BF),
    ]
    outs = pl.pallas_call(
        layer_kernel,
        in_specs=[hbm] * 13,
        out_specs=[vmem] * 8,
        out_shape=[vm(o.shape, o.dtype) for o in shapes],
        scratch_shapes=[
            vm((2, TOK), jnp.int32), vm((2, TOK), F32), vm(act, BF), vm((SLOTS, TP * CH), BF),
            vm((TP * CH, 2 * HID), BF), vm((HID, TP * CH), BF), vm(act, BF), vm(act, BF), vm(act, BF),
            vm(act, BF), vm((3, CH), BF), vm((TP * CH, CH), BF),
            vm(act, BF), vm((SLOTS, TOK), BF), vm((SLOTS, TOK), F32), vm((SLOTS, CH), BF),
            vm((SLOTS, CH), BF), vm((TP, SLOTS, CH), BF), vm((SLOTS, HID), F32), vm((SLOTS, HID), F32),
            vm((SLOTS, HID), BF), vm((SLOTS, 2 * HID), BF),
            vm((TP, SLOTS, CH), BF), vm((2, SLOTS, CH), BF), vm((SLOTS, CH), BF), vm((SLOTS, CH), BF),
            vm((SLOTS, CH), BF), vm(act, BF), vm(act, BF), vm(act, BF), vm(act, BF),
            vm((TP,) + act, BF), vm(act, BF), vm((16, CH), BF), vm((16, CH), BF),
            vm((C, Z, Y) + act, BF), vm((TP, GROUP, ROWS, TOK), BF), vm((SP, ROWS, TOK), BF),
            dma((13,)), dma((2,)), dma((2,)), dma((Z,)), dma((Z,)), dma((2, Z)), dma((2, Z)),
            dma((2, Z)), dma((2, Z)), dma((2,)), dma((2,)), dma((2,)), dma((2, 2)), dma((2, 2)), dma((2, 2)),
            dma((4,)), dma((4, 4)), dma((4, 4)), dma((2,)), dma((1,)), dma((Z,)),
        ],
        compiler_params=pltpu.CompilerParams(
            collective_id=0, has_side_effects=True, vmem_limit_bytes=52428800
        ),
    )(
        route_ids.T, route_weight.T, out_grad, expert_inputs[0], gate_weight[0], up_weight[0],
        down_weight[0], out_gate, in_gate, values, conv_out, conv_taps, proj_weight,
    )
    resid, ogg, igg, vg, proj, gate_grad, up_grad, down_grad = pl.pallas_call(
        flush_kernel,
        in_specs=[vmem] * 8,
        out_specs=[hbm] * 8,
        out_shape=shapes,
        scratch_shapes=[dma((8, 4))],
        compiler_params=pltpu.CompilerParams(vmem_limit_bytes=1024 * 1024),
    )(*outs)
    return resid, ogg, igg, vg, proj, gate_grad[None], up_grad[None], down_grad[None]


def solution(mesh):
    return jax.shard_map(
        per_device,
        mesh=mesh,
        in_specs=(
            P("sp", "tp"), P("sp", None), P("sp", None), P("sp", None, None), P("sp", None, "tp"),
            P("sp", None, "tp"), P("sp", "tp", None), P("sp", "tp"), P("sp", "tp"), P("sp", "tp"),
            P("sp", "tp"), P(None, "tp"), P(None, "tp"),
        ),
        out_specs=(
            P("sp", "tp"), P("sp", "tp"), P("sp", "tp"), P("sp", "tp"), P("sp", "tp"),
            P("sp", None, "tp"), P("sp", None, "tp"), P("sp", "tp", None),
        ),
        check_vma=False,
    )
```

```python
import functools
import math

import jax
import jax.numpy as jnp
from jax import lax
from jax.experimental import pallas as pl
from jax.experimental.pallas import tpu as pltpu
from jax.sharding import PartitionSpec as P

MESH = pl.DeviceIdType.MESH
BF = jnp.bfloat16
F32 = jnp.float32

Z, Y, C = 4, 4, 2
SP = Z * Y * C
TP = 4
TOK = 128
CAP = 16
SLOTS = SP * CAP
CH = 512
HID = 768
ROWS = 64
GROUP = Y * C
CHUNK = GROUP * CAP
ORDER = (0, 2, 1, 3)
FAR_FIRST = (2, 1, 3, 0)


def mm(a, b, dims):
    return lax.dot_general(a, b, ((dims[:1], dims[1:]), ((), ())), preferred_element_type=F32)


def at(block, size):
    return pl.ds(pl.multiple_of(block * size, size), size)


def layer_kernel(
    ids_hbm, w_hbm, og_hbm, inp_hbm, gw_hbm, uw_hbm, dw_hbm,
    gate_hbm, ing_hbm, val_hbm, conv_hbm, taps_hbm, pw_hbm,
    resid_v, ogg_v, igg_v, vg_v, proj_v, gate_grad_v, up_grad_v, down_grad_v,
    ids_v, w_v, og_v, inp_v, gu_v, dw_v, gate_v, ing_v, val_v, conv_v, taps_v, pw_v,
    ogopp_v, disp_v, wslot_v, out0_v, out2_v, r_v, s_v, a_v, hid_v, dgu_v,
    p_v, rp_v, b0_v, ret0_v, ret2_v, m2_v, r2_v, m0_v, rm0_v, rf_v, cg_v, before_v, after_v,
    zall_v, rft_v, rt_v,
    ld_sem, ogopp_sem, disp_sem, recv0_sem, recv2_sem, x_send, x_recv,
    pn_send, pn_recv, ret_send, ret_recv, m2_sem, m0_sem, rf_send, rf_recv, halo_sem, za_send, za_recv,
    zd_sem, rt_send, rt_recv,
):
    sp = lax.axis_index("sp")
    x = lax.axis_index("tp")
    z = sp // GROUP
    inner = lax.rem(sp, GROUP)
    core = lax.rem(sp, C)
    chip = sp // C
    y = lax.rem(chip, Y)
    xp, xm, xo = lax.rem(x + 1, TP), lax.rem(x + 3, TP), lax.rem(x + 2, TP)

    def load(i, src, dst):
        copy = pltpu.make_async_copy(src, dst, ld_sem.at[i])
        copy.start()
        return copy

    def blocks(i, pairs):
        for j in range(TP):
            for src, dst in pairs(at(lax.rem(x + j, TP), CH), pl.ds(j * CH, CH)):
                load(i, src, dst)

    loads = {
        0: load(0, ids_hbm, ids_v),
        1: load(1, w_hbm, w_v),
        2: load(2, og_hbm, og_v),
    }
    load(7, gate_hbm, gate_v)
    load(7, conv_hbm, conv_v)
    load(7, ing_hbm, ing_v)
    load(7, val_hbm, val_v)
    blocks(3, lambda theirs, ours: [(inp_hbm.at[:, theirs], inp_v.at[:, ours])])
    blocks(4, lambda theirs, ours: [
        (gw_hbm.at[theirs, :], gu_v.at[ours, pl.ds(0, HID)]),
        (uw_hbm.at[theirs, :], gu_v.at[ours, pl.ds(HID, HID)]),
    ])
    blocks(6, lambda theirs, ours: [(dw_hbm.at[:, theirs], dw_v.at[:, ours])])
    loads |= {
        9: load(5, pw_hbm, pw_v),
        12: load(8, taps_hbm, taps_v),
    }

    def await_bytes(ref, sem):
        pltpu.make_async_copy(ref, ref, sem).wait()


    barrier = pltpu.get_barrier_semaphore()

    def greet(i, carry):
        other = lax.rem(sp + 1 + i, SP)
        pl.semaphore_signal(barrier, inc=1, device_id=(other, x), device_id_type=MESH)
        return carry

    lax.fori_loop(0, SP - 1, greet, 0)
    for t in (xp, xm, xo):
        pl.semaphore_signal(barrier, inc=1, device_id=(sp, t), device_id_type=MESH)

    with jax.named_scope("w_load"):
        loads[0].wait()
        loads[1].wait()
        loads[2].wait()
    ids = ids_v[...]
    wts = w_v[...]
    e_iota = lax.broadcasted_iota(jnp.int32, (SP, TOK), 0)
    first = e_iota == ids[0:1, :]
    second = e_iota == ids[1:2, :]
    named = jnp.where(first | second, 1.0, 0.0)
    w_et = jnp.where(first, wts[0:1, :], 0.0) + jnp.where(second, wts[1:2, :], 0.0)
    earlier = lax.broadcasted_iota(jnp.int32, (TOK, TOK), 0) < lax.broadcasted_iota(
        jnp.int32, (TOK, TOK), 1
    )
    prefix = mm(named.astype(BF), jnp.where(earlier, 1.0, 0.0).astype(BF), (1, 0))
    rank = jnp.where(named > 0.5, prefix, -1.0)
    r_iota = lax.broadcasted_iota(jnp.int32, (SP, CAP, TOK), 1).astype(F32)
    hit = jnp.broadcast_to(rank[:, None, :], (SP, CAP, TOK)) == r_iota
    disp = jnp.where(hit, 1.0, 0.0)
    wslot = jnp.sum(disp * w_et[:, None, :], axis=2, keepdims=True)
    disp_v[...] = disp.reshape(SLOTS, TOK).astype(BF)
    wslot_v[...] = jnp.broadcast_to(wslot, (SP, CAP, TOK)).reshape(SLOTS, TOK)

    def dispatch(tok_ref, out_ref):
        rows = mm(disp_v[...], tok_ref[...], (1, 0))
        out_ref[...] = (rows * jnp.tile(wslot_v[...], (1, CH // TOK))).astype(BF)

    dispatch(og_v, out0_v)
    TILE = 256

    def hidden_tile(n):
        cols = slice(n * TILE, (n + 1) * TILE)
        ups = slice(HID + n * TILE, HID + (n + 1) * TILE)

        def rows_of(m, carry):
            rows = at(m, 256)
            pre_gate = mm(inp_v[rows, :], gu_v[:, cols], (1, 0))
            pre_up = mm(inp_v[rows, :], gu_v[:, ups], (1, 0))
            sig = 1.0 / (1.0 + jnp.exp(-pre_gate))
            act = pre_gate * sig
            s_v[rows, cols] = act
            a_v[rows, cols] = pre_up * sig * (1.0 + pre_gate * (1.0 - sig))
            hid_v[rows, cols] = (act * pre_up).astype(BF)
            return carry

        lax.fori_loop(0, SLOTS // 256, rows_of, 0)

    with jax.named_scope("w_barrier"):
        pl.semaphore_wait(barrier, SP - 1 + TP - 1)

    ogopp = pltpu.make_async_remote_copy(
        og_v, ogopp_v, ogopp_sem.at[0], ogopp_sem.at[1], device_id=(sp, xo), device_id_type=MESH
    )
    ogopp.start()

    def plane(zz, skip_self):
        peers = []
        for dy in FAR_FIRST:
            for dc in (1, 0):
                if not (skip_self and dy == 0 and dc == 0):
                    peers.append((zz * Y + lax.rem(y + dy, Y)) * C + lax.rem(core + dc, C))
        return peers

    def interleaved(dzs, sign):
        lists = [[(dz, there) for there in plane(lax.rem(z + sign * dz + Z, Z), dz == 0)] for dz in dzs]
        return [entry for i in range(GROUP) for entries in lists for entry in entries[i : i + 1]]

    def scatter(out_ref, block, which, recv_sem, dzs):
        if 0 in dzs:
            r_v[block, at(sp, CAP), :] = out_ref[at(sp, CAP), :]
        for dz, there in interleaved(dzs, -1):
            pltpu.make_async_remote_copy(
                out_ref.at[at(there, CAP), :],
                r_v.at[block, at(sp, CAP), :],
                disp_sem.at[which],
                recv_sem.at[dz],
                device_id=(there, x),
                device_id_type=MESH,
            ).start()

    def chunk_rows(dz):
        return at(lax.rem(z + dz, Z), CHUNK)

    r_v[0, at(sp, CAP), :] = out0_v[at(sp, CAP), :]
    for dy in (1, 3, 0, 2):
        for dc in (1, 0) if dy else (1,):
            there = (z * Y + lax.rem(y + dy, Y)) * C + lax.rem(core + dc, C)
            pltpu.make_async_remote_copy(
                out0_v.at[at(there, CAP), :],
                r_v.at[0, at(sp, CAP), :],
                disp_sem.at[0],
                recv0_sem.at[Z if dy == 2 else 0],
                device_id=(there, x),
                device_id_type=MESH,
            ).start()
    scatter(out0_v, 0, 0, recv0_sem, (2,))
    scatter(out0_v, 0, 0, recv0_sem, (1, 3))

    def await_group(block, dz, recv_sem):
        count = CHUNK - CAP if dz == 0 else CHUNK
        with jax.named_scope(f"w_group{block}_{dz}"):
            await_bytes(r_v.at[block, pl.ds(0, count), :], recv_sem.at[dz])

    def forward_rows(k, rows):
        for way, (there, landing) in enumerate(((xp, 3), (xm, 1))):
            copy = pltpu.make_async_remote_copy(
                r_v.at[0, rows, :],
                r_v.at[landing, rows, :],
                x_send.at[0],
                x_recv.at[k],
                device_id=(sp, there),
                device_id_type=MESH,
            )
            copy.start()

    def forward_first():
        near = C * CAP
        with jax.named_scope("w_group0_0"):
            await_bytes(r_v.at[0, pl.ds(0, 3 * near - CAP), :], recv0_sem.at[0])
        for dy in (0, 1, 3):
            forward_rows(0, at(z * Y + lax.rem(y + dy, Y), near))
        with jax.named_scope("w_group0_far"):
            await_bytes(r_v.at[0, pl.ds(0, near), :], recv0_sem.at[Z])
        forward_rows(0, at(z * Y + lax.rem(y + 2, Y), near))

    def forward(k):
        await_group(0, ORDER[k], recv0_sem)
        forward_rows(k, chunk_rows(ORDER[k]))

    await_bytes(rf_v, ld_sem.at[7])
    gate_vals = gate_v[...].astype(F32)
    conv_vals = conv_v[...].astype(F32)
    zall_v[core, z, y] = (gate_vals * conv_vals).astype(BF)
    partner = sp + 1 - 2 * core
    zp, zm = lax.rem(z + 1, Z), lax.rem(z + 3, Z)
    yp, ym = lax.rem(y + 1, Y), lax.rem(y + 3, Y)
    west, east = pl.ds(0, CH // 2), pl.ds(CH // 2, CH // 2)
    low, high, full = pl.ds(0, TOK // 2), pl.ds(TOK // 2, TOK // 2), pl.ds(0, TOK)
    every = pl.ds(0, Z)

    def spread_arrived(phase):
        rows = (2 * TOK, TOK, 8 * TOK, 4 * TOK)[phase]
        with jax.named_scope(f"w_spread{phase + 1}"):
            await_bytes(r_v.at[pl.ds(0, rows // TOK), pl.ds(0, TOK), :] if rows <= 2 * TOK else r_v.at[pl.ds(0, 2), pl.ds(0, rows // 2), :], za_recv.at[phase])

    def spread(phase):
        steps = (
            ((z, y, full, west), (z, y, full, west), (z, y, full, east), (z, y, full, east)),
            ((z, ym, low, west), (z, yp, high, west), (zm, y, low, east), (zp, y, high, east)),
            ((z, every, full, west), (z, every, full, west), (every, y, full, east), (every, y, full, east)),
            ((zm, every, low, west), (zp, every, high, west), (every, ym, low, east), (every, yp, high, east)),
        )[phase]
        along_y, along_z = ((z, yp), (z, ym)), ((zp, y), (zm, y))
        theres = along_y + along_z if phase < 2 else along_z + along_y
        if phase > 0:
            spread_arrived(phase - 1)
        for (bz, by, rows, cols), (tz, ty) in zip(steps, theres):
            part = zall_v.at[core, bz, by, rows, cols]
            copy = pltpu.make_async_remote_copy(
                part, part, za_send.at[0], za_recv.at[phase],
                device_id=((tz * Y + ty) * C + core, x), device_id_type=MESH,
            )
            copy.start()

    spread(0)
    with jax.named_scope("w_weights"):
        await_bytes(inp_v, ld_sem.at[3])
        await_bytes(gu_v, ld_sem.at[4])
    hidden_tile(0)
    hidden_tile(1)
    forward_first()
    with jax.named_scope("w_ogopp"):
        ogopp.wait_recv()
    dispatch(ogopp_v, out2_v)
    scatter(out2_v, 2, 1, recv2_sem, (2, 0))
    forward(1)
    hidden_tile(2)
    spread(1)
    scatter(out2_v, 2, 1, recv2_sem, (1, 3))
    forward(2)
    forward(3)
    await_bytes(dw_v, ld_sem.at[6])

    def give_back(src_ref, dst_ref, which, dzs):
        if 0 in dzs:
            dst_ref[at(sp, CAP), :] = src_ref[at(sp, CAP), :]
        give_rows(src_ref, dst_ref, which, [there for _, there in interleaved(dzs, 1)])

    def give_rows(src_ref, dst_ref, which, theres):
        for there in theres:
            pltpu.make_async_remote_copy(
                src_ref.at[at(there, CAP), :],
                dst_ref.at[at(sp, CAP), :],
                ret_send.at[which],
                ret_recv.at[which],
                device_id=(there, x),
                device_id_type=MESH,
            ).start()

    HALF = GROUP // 2

    def half_plane(zz, h):
        return [
            (zz * Y + 2 * h + lax.rem(y + dy, 2)) * C + lax.rem(core + dc, C)
            for dy in (1, 0)
            for dc in (1, 0)
        ]

    def pieces(k):
        if k < 2:
            return [(k, chunk_rows(ORDER[k]), CHUNK)]
        h = k - 2
        return [
            (2 * k - 2 + i, at(lax.rem(z + dz, Z) * 2 + h, CHUNK // 2), CHUNK // 2)
            for i, dz in enumerate(ORDER[2:])
        ]

    def finish_own(k):
        with jax.named_scope(f"w_part{k}"):
            await_bytes(rp_v.at[:, pl.ds(0, CHUNK), :], pn_recv.at[k])
        for _, rows, _ in pieces(k):
            total = p_v[0, rows, :].astype(F32) + rp_v[0, rows, :].astype(F32) + rp_v[1, rows, :].astype(F32)
            b0_v[rows, :] = total.astype(BF)
        if k < 2:
            give_back(b0_v, ret0_v, 0, (ORDER[k],))
        else:
            lists = [half_plane(lax.rem(z + dz, Z), k - 2) for dz in ORDER[2:]]
            give_rows(b0_v, ret0_v, 0, [there for pair in zip(*lists) for there in pair])

    def rows_pair(ref, halves):
        return jnp.concatenate([ref[rows, :] for _, rows, _ in halves], axis=0)

    def put_pair(ref, halves, value):
        start = 0
        for _, rows, size in halves:
            ref[rows, :] = value[start : start + size, :]
            start += size

    for ks in ((0, 1), (2, 3)):
        halves = [piece for k in ks for piece in pieces(k)]
        for k in ks:
            await_group(2, ORDER[k], recv2_sem)
            with jax.named_scope(f"w_x{k}"):
                await_bytes(r_v.at[pl.ds(0, 2), pl.ds(0, CHUNK), :], x_recv.at[k])
        left = jnp.concatenate([rows_pair(r_v.at[j], halves) for j in range(TP)], axis=1)
        d_hidden = mm(left, dw_v[...], (1, 1))
        if ks[0] == 0:
            spread(2)
        put_pair(dgu_v.at[:, pl.ds(0, HID)], halves, (d_hidden * rows_pair(a_v, halves)).astype(BF))
        put_pair(dgu_v.at[:, pl.ds(HID, HID)], halves, (d_hidden * rows_pair(s_v, halves)).astype(BF))
        for j in (1, 3, 2, 0):
            part = mm(rows_pair(dgu_v, halves), gu_v[j * CH : (j + 1) * CH, :], (1, 1))
            put_pair(p_v.at[j], halves, part.astype(BF))
            if j in (1, 3):
                way = 0 if j == 1 else 1
                for i, rows, _ in halves:
                    copy = pltpu.make_async_remote_copy(
                        p_v.at[j, rows, :],
                        rp_v.at[way, rows, :],
                        pn_send.at[0],
                        pn_recv.at[i if i < 2 else i // 2 + 1],
                        device_id=(sp, xp if j == 1 else xm),
                        device_id_type=MESH,
                    )
                    copy.start()
            if j == 2:
                give_back(p_v.at[2], ret2_v, 1, [ORDER[k] for k in ks])
    finish_own(0)
    finish_own(1)

    slot_scale = 1.0 / math.sqrt(SLOTS)

    def down_tiles(lower, upper):
        def tile(n, carry):
            rows = at(n, 256)
            turned = hid_v[:, rows].T
            for j in range(TP):
                part = mm(turned, r_v[j], (1, 0)) * slot_scale
                down_grad_v[rows, at(lax.rem(x + j, TP), CH)] = part.astype(BF)
            return carry

        lax.fori_loop(lower, upper, tile, 0)

    def gate_tiles(lower, upper):
        def tile(n, carry):
            rows = at(n, 256)
            turned = inp_v[:, rows].T
            rows = at(lax.rem(x + n // 2, TP) * 2 + lax.rem(n, 2), 256)
            gate_grad_v[rows, :] = (mm(turned, dgu_v[:, 0:HID], (1, 0)) * slot_scale).astype(BF)
            up_grad_v[rows, :] = (mm(turned, dgu_v[:, HID : 2 * HID], (1, 0)) * slot_scale).astype(BF)
            return carry

        lax.fori_loop(lower, upper, tile, 0)

    finish_own(2)
    finish_own(3)
    spread(3)

    def await_returned(ref, which):
        with jax.named_scope(f"w_ret{which}"):
            await_bytes(ref.at[pl.ds(0, SLOTS - CAP), :], ret_recv.at[which])

    def to_opposite(src, dst, send_sem, recv_sem):
        copy = pltpu.make_async_remote_copy(
            src, dst, send_sem, recv_sem, device_id=(sp, xo), device_id_type=MESH
        )
        copy.start()
        return copy

    await_returned(ret2_v, 1)
    m2_v[...] = mm(disp_v[...], ret2_v[...], (0, 0)).astype(BF)
    m2 = to_opposite(m2_v, r2_v, m2_sem.at[0], m2_sem.at[1])
    with jax.named_scope("g_gate"):
        gate_tiles(0, 4)
    await_returned(ret0_v, 0)
    moe = mm(disp_v[...], ret0_v[...], (0, 0))
    m0_v[...] = moe.astype(BF)
    m0 = {}

    def lanes(s):
        return at(lax.rem(y + s, Y), TOK)

    def send_m0(s):
        m0[s] = to_opposite(m0_v.at[:, lanes(s)], rm0_v.at[:, lanes(s)], m0_sem.at[Y], m0_sem.at[s])

    send_m0(2)
    send_m0(0)
    with jax.named_scope("w_m2"):
        m2.wait_recv()
    own = (og_v[...].astype(F32) + moe + r2_v[...].astype(F32)).astype(BF)
    rf_v[0] = own
    rf_copies = {}

    def send_rf(s):
        for there, landing in ((xp, 3), (xm, 1)):
            copy = pltpu.make_async_remote_copy(
                rf_v.at[0, :, lanes(s)],
                rf_v.at[landing, :, lanes(s)],
                rf_send.at[0],
                rf_recv.at[landing // 2, s],
                device_id=(sp, there),
                device_id_type=MESH,
            )
            copy.start()
            rf_copies[landing, s] = copy

    send_rf(2)
    send_rf(0)
    send_m0(1)
    send_m0(3)
    send_rf(1)
    send_rf(3)
    resid_v[...] = own
    loads[9].wait()

    def mix_part(j):
        return mm(rf_v[j], pw_v[at(lax.rem(x + j, TP), CH), :], (1, 0))

    def order_of(cc, zz, yy):
        return (cc * Z + zz) * Y + yy

    mine = order_of(core, z, y)

    def share(j, s):
        block = lax.rem(x + j, TP)
        across = lax.rem(y + s, Y)
        rft_v[j, across] = rf_v[j, :, lanes(s)].T.reshape(C, ROWS, TOK)
        for dc in (1, 0):
            inside = lax.rem(core + dc, C)
            there = (block * Y + across) * C + inside

            @pl.when(there != sp)
            def _():
                pltpu.make_async_remote_copy(
                    rft_v.at[j, across, inside],
                    rt_v.at[mine],
                    rt_send.at[0],
                    rt_recv.at[lax.rem(z - block + Z, Z)],
                    device_id=(there, x),
                    device_id_type=MESH,
                ).start()

    for s in (2, 0, 1, 3):
        share(0, s)
    mix = mix_part(0)
    with jax.named_scope("g_gate2"):
        gate_tiles(4, 8)
    spread_arrived(3)
    to_partner = pltpu.make_async_remote_copy(
        zall_v.at[core], zall_v.at[core], zd_sem.at[0], zd_sem.at[1],
        device_id=(partner, x), device_id_type=MESH,
    )
    to_partner.start()
    for s in (2, 0, 1, 3):
        for j in (3, 1):
            with jax.named_scope(f"w_rf{j}_{s}"):
                rf_copies[j, s].wait_recv()
            share(j, s)
        with jax.named_scope(f"w_rf2_{s}"):
            m0[s].wait_recv()
        cols = lanes(s)
        other = ogopp_v[:, cols].astype(F32) + rm0_v[:, cols].astype(F32) + m2_v[:, cols].astype(F32)
        rf_v[2, :, cols] = other.astype(BF)
        if s in (2, 0):
            share(2, s)
    for j in (3, 1, 2):
        mix = mix + mix_part(j)
    ogg_v[...] = (mix * conv_vals).astype(BF)
    cg_v[...] = (mix * gate_vals).astype(BF)
    down = pltpu.make_async_remote_copy(
        cg_v.at[pl.ds(0, 16), :], after_v, halo_sem.at[0], halo_sem.at[1],
        device_id=(lax.rem(sp + SP - 1, SP), x), device_id_type=MESH,
    )
    up = pltpu.make_async_remote_copy(
        cg_v.at[pl.ds(TOK - 16, 16), :], before_v, halo_sem.at[2], halo_sem.at[3],
        device_id=(lax.rem(sp + 1, SP), x), device_id_type=MESH,
    )
    down.start()
    up.start()
    share(2, 1)
    share(2, 3)
    rt_v[mine] = rft_v[lax.rem(z - x + TP, TP), y, core]
    with jax.named_scope("g_down"):
        down_tiles(0, HID // 256)
    ogopp.wait_send()
    for which, ref in ((0, out0_v), (1, out2_v)):
        await_bytes(ref.at[pl.ds(0, SLOTS - CAP), :], disp_sem.at[which])
        await_bytes(ref.at[pl.ds(0, SLOTS - CAP), :], ret_send.at[which])
    m2.wait_send()
    await_bytes(r_v.at[pl.ds(0, 2)], x_send.at[0])
    await_bytes(r_v.at[pl.ds(0, 2)], pn_send.at[0])
    with jax.named_scope("w_zd"):
        to_partner.wait_recv()

    def proj_group(dz):
        count = GROUP - 1 if dz == 0 else GROUP
        with jax.named_scope(f"w_rt{dz}"):
            await_bytes(rt_v.at[pl.ds(0, count)], rt_recv.at[dz])
        zz = lax.rem(z + dz, Z)
        total = None
        for cc in range(C):
            left = jnp.concatenate([rt_v[order_of(cc, zz, yy)] for yy in range(Y)], axis=1)
            term = mm(left, zall_v[cc, zz].reshape(Y * TOK, CH), (1, 0))
            total = term if total is None else total + term
        return total

    proj = proj_group(0) + proj_group(1)

    loads[12].wait()
    with jax.named_scope("w_halo"):
        down.wait_recv()
        up.wait_recv()
    cg = cg_v[...].astype(F32)
    taps = taps_v[...].astype(F32)
    row = lax.broadcasted_iota(jnp.int32, (TOK, CH), 0)
    has_before = jnp.where(sp > 0, 1.0, 0.0)
    has_after = jnp.where(sp < SP - 1, 1.0, 0.0)
    before = before_v[...].astype(F32)[15:16, :] * has_before
    after = after_v[...].astype(F32)[0:1, :] * has_after
    nxt = jnp.where(row == TOK - 1, jnp.broadcast_to(after, (TOK, CH)), pltpu.roll(cg, TOK - 1, 0))
    prv = jnp.where(row == 0, jnp.broadcast_to(before, (TOK, CH)), pltpu.roll(cg, 1, 0))
    value_grad = nxt * taps[0:1, :] + cg * taps[1:2, :] + prv * taps[2:3, :]
    igg_v[...] = (value_grad * val_v[...].astype(F32)).astype(BF)
    vg_v[...] = (value_grad * ing_v[...].astype(F32)).astype(BF)

    proj = proj + proj_group(3)
    proj = proj + proj_group(2)
    proj_v[...] = proj * (1.0 / math.sqrt(TOK * SP))

    await_bytes(r_v.at[:, pl.ds(0, 15 * TOK // TP), :], za_send.at[0])
    to_partner.wait_send()
    await_bytes(m0_v, m0_sem.at[Y])
    await_bytes(rf_v.at[pl.ds(0, 2)], rf_send.at[0])
    down.wait_send()
    up.wait_send()
    await_bytes(rt_v.at[pl.ds(0, SP - 1)], rt_send.at[0])


def flush_kernel(*refs):
    count = (len(refs) - 1) // 2
    sems = refs[-1]
    for i in reversed(range(count)):
        src, dst = refs[i], refs[count + i]
        pieces = 4 if i >= count - 3 else 1
        rows = src.shape[0] // pieces
        for p in range(pieces):
            part = pl.ds(p * rows, rows)
            pltpu.make_async_copy(src.at[part, :], dst.at[part, :], sems.at[i]).start()
    for i in range(count):
        pltpu.make_async_copy(refs[i], refs[count + i], sems.at[i]).wait()


def per_device(
    out_grad, route_ids, route_weight, expert_inputs, gate_weight, up_weight, down_weight,
    out_gate, in_gate, values, conv_out, conv_taps, proj_weight,
):
    sds = jax.ShapeDtypeStruct
    hbm = pl.BlockSpec(memory_space=pltpu.HBM)
    vm = pltpu.VMEM
    dma = pltpu.SemaphoreType.DMA
    act = (TOK, CH)
    vmem = pl.BlockSpec(memory_space=pltpu.VMEM)
    shapes = [
        sds(act, BF), sds(act, BF), sds(act, BF), sds(act, BF), sds((ROWS, CH), F32),
        sds((TP * CH, HID), BF), sds((TP * CH, HID), BF), sds((HID, TP * CH), BF),
    ]
    outs = pl.pallas_call(
        layer_kernel,
        in_specs=[hbm] * 13,
        out_specs=[vmem] * 8,
        out_shape=[vm(o.shape, o.dtype) for o in shapes],
        scratch_shapes=[
            vm((2, TOK), jnp.int32), vm((2, TOK), F32), vm(act, BF), vm((SLOTS, TP * CH), BF),
            vm((TP * CH, 2 * HID), BF), vm((HID, TP * CH), BF), vm(act, BF), vm(act, BF), vm(act, BF),
            vm(act, BF), vm((3, CH), BF), vm((TP * CH, CH), BF),
            vm(act, BF), vm((SLOTS, TOK), BF), vm((SLOTS, TOK), F32), vm((SLOTS, CH), BF),
            vm((SLOTS, CH), BF), vm((TP, SLOTS, CH), BF), vm((SLOTS, HID), F32), vm((SLOTS, HID), F32),
            vm((SLOTS, HID), BF), vm((SLOTS, 2 * HID), BF),
            vm((TP, SLOTS, CH), BF), vm((2, SLOTS, CH), BF), vm((SLOTS, CH), BF), vm((SLOTS, CH), BF),
            vm((SLOTS, CH), BF), vm(act, BF), vm(act, BF), vm(act, BF), vm(act, BF),
            vm((TP,) + act, BF), vm(act, BF), vm((16, CH), BF), vm((16, CH), BF),
            vm((C, Z, Y) + act, BF), vm((TP, Y, C, ROWS, TOK), BF), vm((SP, ROWS, TOK), BF),
            dma((9,)), dma((2,)), dma((2,)), dma((Z + 1,)), dma((Z,)), dma((1,)), dma((Z,)),
            dma((1,)), dma((Z,)), dma((2,)), dma((2,)), dma((2,)), dma((Y + 1,)), dma((1,)), dma((2, Y)),
            dma((4,)), dma((1,)), dma((4,)), dma((2,)), dma((1,)), dma((Z,)),
        ],
        compiler_params=pltpu.CompilerParams(
            collective_id=0, has_side_effects=True, vmem_limit_bytes=52428800
        ),
    )(
        route_ids.T, route_weight.T, out_grad, expert_inputs[0], gate_weight[0], up_weight[0],
        down_weight[0], out_gate, in_gate, values, conv_out, conv_taps, proj_weight,
    )
    resid, ogg, igg, vg, proj, gate_grad, up_grad, down_grad = pl.pallas_call(
        flush_kernel,
        in_specs=[vmem] * 8,
        out_specs=[hbm] * 8,
        out_shape=shapes,
        scratch_shapes=[dma((8,))],
        compiler_params=pltpu.CompilerParams(vmem_limit_bytes=1024 * 1024),
    )(*outs)
    return resid, ogg, igg, vg, proj, gate_grad[None], up_grad[None], down_grad[None]


def solution(mesh):
    return jax.shard_map(
        per_device,
        mesh=mesh,
        in_specs=(
            P("sp", "tp"), P("sp", None), P("sp", None), P("sp", None, None), P("sp", None, "tp"),
            P("sp", None, "tp"), P("sp", "tp", None), P("sp", "tp"), P("sp", "tp"), P("sp", "tp"),
            P("sp", "tp"), P(None, "tp"), P(None, "tp"),
        ),
        out_specs=(
            P("sp", "tp"), P("sp", "tp"), P("sp", "tp"), P("sp", "tp"), P("sp", "tp"),
            P("sp", None, "tp"), P("sp", None, "tp"), P("sp", "tp", None),
        ),
        check_vma=False,
    )
```

```python
import functools
import math

import jax
import jax.numpy as jnp
from jax import lax
from jax.experimental import pallas as pl
from jax.experimental.pallas import tpu as pltpu
from jax.sharding import PartitionSpec as P

MESH = pl.DeviceIdType.MESH
BF = jnp.bfloat16
F32 = jnp.float32

Z, Y, C = 4, 4, 2
SP = Z * Y * C
TP = 4
TOK = 128
CAP = 16
SLOTS = SP * CAP
CH = 512
HID = 768
ROWS = 64
GROUP = Y * C
CHUNK = GROUP * CAP
ORDER = (0, 2, 1, 3)
FAR_FIRST = (2, 1, 3, 0)


def mm(a, b, dims):
    return lax.dot_general(a, b, ((dims[:1], dims[1:]), ((), ())), preferred_element_type=F32)


def at(block, size):
    return pl.ds(pl.multiple_of(block * size, size), size)


def layer_kernel(
    ids_hbm, w_hbm, og_hbm, inp_hbm, gw_hbm, uw_hbm, dw_hbm,
    gate_hbm, ing_hbm, val_hbm, conv_hbm, taps_hbm, pw_hbm,
    resid_v, ogg_v, igg_v, vg_v, proj_v, gate_grad_v, up_grad_v, down_grad_v,
    ids_v, w_v, og_v, inp_v, gu_v, dw_v, gate_v, ing_v, val_v, conv_v, taps_v, pw_v,
    ogopp_v, disp_v, wslot_v, out0_v, out2_v, r_v, s_v, a_v, hid_v, dgu_v,
    p_v, rp_v, b0_v, ret0_v, ret2_v, m2_v, r2_v, m0_v, rm0_v, rf_v, cg_v, before_v, after_v,
    zall_v, rft_v, rt_v,
    ld_sem, ogopp_sem, disp_sem, recv0_sem, recv2_sem, x_send, x_recv,
    pn_send, pn_recv, ret_send, ret_recv, m2_sem, m0_sem, rf_send, rf_recv, halo_sem, za_send, za_recv,
    zd_sem, rt_send, rt_recv,
):
    sp = lax.axis_index("sp")
    x = lax.axis_index("tp")
    z = sp // GROUP
    inner = lax.rem(sp, GROUP)
    core = lax.rem(sp, C)
    chip = sp // C
    y = lax.rem(chip, Y)
    xp, xm, xo = lax.rem(x + 1, TP), lax.rem(x + 3, TP), lax.rem(x + 2, TP)

    def load(i, src, dst):
        copy = pltpu.make_async_copy(src, dst, ld_sem.at[i])
        copy.start()
        return copy

    first_loads = {
        0: load(0, ids_hbm, ids_v),
        1: load(1, w_hbm, w_v),
        2: load(2, og_hbm, og_v),
    }
    barrier = pltpu.get_barrier_semaphore()

    def greet(s, t):
        pl.semaphore_signal(barrier, inc=1, device_id=(s, t), device_id_type=MESH)

    for dz in FAR_FIRST:
        for dy in FAR_FIRST:
            for dc in (1, 0):
                if dz or dy or dc:
                    chip_there = lax.rem(z + dz, Z) * Y + lax.rem(y + dy, Y)
                    greet(chip_there * C + lax.rem(core + dc, C), x)
        if dz == 2:
            for t in (xo, xp, xm):
                greet(sp, t)

    def blocks(i, pairs):
        for j in range(TP):
            for src, dst in pairs(at(lax.rem(x + j, TP), CH), pl.ds(j * CH, CH)):
                load(i, src, dst)

    loads = first_loads
    load(7, gate_hbm, gate_v)
    load(7, conv_hbm, conv_v)
    load(7, ing_hbm, ing_v)
    load(7, val_hbm, val_v)
    blocks(3, lambda theirs, ours: [(inp_hbm.at[:, theirs], inp_v.at[:, ours])])
    blocks(4, lambda theirs, ours: [
        (gw_hbm.at[theirs, :], gu_v.at[ours, pl.ds(0, HID)]),
        (uw_hbm.at[theirs, :], gu_v.at[ours, pl.ds(HID, HID)]),
    ])
    blocks(6, lambda theirs, ours: [(dw_hbm.at[:, theirs], dw_v.at[:, ours])])
    loads |= {
        9: load(5, pw_hbm, pw_v),
        12: load(8, taps_hbm, taps_v),
    }

    def await_bytes(ref, sem):
        pltpu.make_async_copy(ref, ref, sem).wait()


    with jax.named_scope("w_load"):
        loads[0].wait()
        loads[1].wait()
        loads[2].wait()
    ids = ids_v[...]
    wts = w_v[...]
    e_iota = lax.broadcasted_iota(jnp.int32, (SP, TOK), 0)
    first = e_iota == ids[0:1, :]
    second = e_iota == ids[1:2, :]
    named = jnp.where(first | second, 1.0, 0.0)
    w_et = jnp.where(first, wts[0:1, :], 0.0) + jnp.where(second, wts[1:2, :], 0.0)
    earlier = lax.broadcasted_iota(jnp.int32, (TOK, TOK), 0) < lax.broadcasted_iota(
        jnp.int32, (TOK, TOK), 1
    )
    prefix = mm(named.astype(BF), jnp.where(earlier, 1.0, 0.0).astype(BF), (1, 0))
    rank = jnp.where(named > 0.5, prefix, -1.0)
    r_iota = lax.broadcasted_iota(jnp.int32, (SP, CAP, TOK), 1).astype(F32)
    hit = jnp.broadcast_to(rank[:, None, :], (SP, CAP, TOK)) == r_iota
    disp = jnp.where(hit, 1.0, 0.0)
    wslot = jnp.sum(disp * w_et[:, None, :], axis=2, keepdims=True)
    disp_v[...] = disp.reshape(SLOTS, TOK).astype(BF)
    wslot_v[...] = jnp.broadcast_to(wslot, (SP, CAP, TOK)).reshape(SLOTS, TOK)

    def dispatch(tok_ref, out_ref):
        rows = mm(disp_v[...], tok_ref[...], (1, 0))
        out_ref[...] = (rows * jnp.tile(wslot_v[...], (1, CH // TOK))).astype(BF)

    dispatch(og_v, out0_v)
    TILE = 256

    def hidden_tile(n):
        cols = slice(n * TILE, (n + 1) * TILE)
        ups = slice(HID + n * TILE, HID + (n + 1) * TILE)

        def rows_of(m, carry):
            rows = at(m, 256)
            pre_gate = mm(inp_v[rows, :], gu_v[:, cols], (1, 0))
            pre_up = mm(inp_v[rows, :], gu_v[:, ups], (1, 0))
            sig = 1.0 / (1.0 + jnp.exp(-pre_gate))
            act = pre_gate * sig
            s_v[rows, cols] = act
            a_v[rows, cols] = pre_up * sig * (1.0 + pre_gate * (1.0 - sig))
            hid_v[rows, cols] = (act * pre_up).astype(BF)
            return carry

        lax.fori_loop(0, SLOTS // 256, rows_of, 0)

    with jax.named_scope("w_barrier"):
        pl.semaphore_wait(barrier, SP - 1 + TP - 1)

    ogopp = pltpu.make_async_remote_copy(
        og_v, ogopp_v, ogopp_sem.at[0], ogopp_sem.at[1], device_id=(sp, xo), device_id_type=MESH
    )
    ogopp.start()

    def plane(zz, skip_self):
        peers = []
        for dy in FAR_FIRST:
            for dc in (1, 0):
                if not (skip_self and dy == 0 and dc == 0):
                    peers.append((zz * Y + lax.rem(y + dy, Y)) * C + lax.rem(core + dc, C))
        return peers

    def interleaved(dzs, sign):
        lists = [[(dz, there) for there in plane(lax.rem(z + sign * dz + Z, Z), dz == 0)] for dz in dzs]
        return [entry for i in range(GROUP) for entries in lists for entry in entries[i : i + 1]]

    def scatter(out_ref, block, which, recv_sem, dzs):
        if 0 in dzs:
            r_v[block, at(sp, CAP), :] = out_ref[at(sp, CAP), :]
        for dz, there in interleaved(dzs, -1):
            pltpu.make_async_remote_copy(
                out_ref.at[at(there, CAP), :],
                r_v.at[block, at(sp, CAP), :],
                disp_sem.at[which],
                recv_sem.at[dz % 2 if block == 2 else dz],
                device_id=(there, x),
                device_id_type=MESH,
            ).start()

    def chunk_rows(dz):
        return at(lax.rem(z + dz, Z), CHUNK)

    r_v[0, at(sp, CAP), :] = out0_v[at(sp, CAP), :]
    for dy in (1, 3, 0, 2):
        for dc in (1, 0) if dy else (1,):
            there = (z * Y + lax.rem(y + dy, Y)) * C + lax.rem(core + dc, C)
            pltpu.make_async_remote_copy(
                out0_v.at[at(there, CAP), :],
                r_v.at[0, at(sp, CAP), :],
                disp_sem.at[0],
                recv0_sem.at[Z if dy == 2 else 0],
                device_id=(there, x),
                device_id_type=MESH,
            ).start()
    scatter(out0_v, 0, 0, recv0_sem, (2,))
    scatter(out0_v, 0, 0, recv0_sem, (1, 3))

    def await_group(block, dz, recv_sem):
        count = CHUNK - CAP if dz == 0 else CHUNK
        with jax.named_scope(f"w_group{block}_{dz}"):
            await_bytes(r_v.at[block, pl.ds(0, count), :], recv_sem.at[dz])

    def forward_rows(k, rows):
        for way, (there, landing) in enumerate(((xp, 3), (xm, 1))):
            copy = pltpu.make_async_remote_copy(
                r_v.at[0, rows, :],
                r_v.at[landing, rows, :],
                x_send.at[0],
                x_recv.at[k // 2],
                device_id=(sp, there),
                device_id_type=MESH,
            )
            copy.start()

    def forward_first():
        near = C * CAP
        with jax.named_scope("w_group0_0"):
            await_bytes(r_v.at[0, pl.ds(0, 3 * near - CAP), :], recv0_sem.at[0])
        for dy in (0, 1, 3):
            forward_rows(0, at(z * Y + lax.rem(y + dy, Y), near))
        with jax.named_scope("w_group0_far"):
            await_bytes(r_v.at[0, pl.ds(0, near), :], recv0_sem.at[Z])
        forward_rows(0, at(z * Y + lax.rem(y + 2, Y), near))

    def forward(k):
        await_group(0, ORDER[k], recv0_sem)
        forward_rows(k, chunk_rows(ORDER[k]))

    await_bytes(rf_v, ld_sem.at[7])
    gate_vals = gate_v[...].astype(F32)
    conv_vals = conv_v[...].astype(F32)
    zall_v[core, z, y] = (gate_vals * conv_vals).astype(BF)
    partner = sp + 1 - 2 * core
    zp, zm = lax.rem(z + 1, Z), lax.rem(z + 3, Z)
    yp, ym = lax.rem(y + 1, Y), lax.rem(y + 3, Y)
    west, east = pl.ds(0, CH // 2), pl.ds(CH // 2, CH // 2)
    low, high, full = pl.ds(0, TOK // 2), pl.ds(TOK // 2, TOK // 2), pl.ds(0, TOK)
    every = pl.ds(0, Z)

    def spread_arrived(phase):
        rows = (2 * TOK, TOK, 8 * TOK, 4 * TOK)[phase]
        with jax.named_scope(f"w_spread{phase + 1}"):
            await_bytes(r_v.at[pl.ds(0, rows // TOK), pl.ds(0, TOK), :] if rows <= 2 * TOK else r_v.at[pl.ds(0, 2), pl.ds(0, rows // 2), :], za_recv.at[phase])

    def spread(phase):
        steps = (
            ((z, y, full, west), (z, y, full, west), (z, y, full, east), (z, y, full, east)),
            ((z, ym, low, west), (z, yp, high, west), (zm, y, low, east), (zp, y, high, east)),
            ((z, every, full, west), (z, every, full, west), (every, y, full, east), (every, y, full, east)),
            ((zm, every, low, west), (zp, every, high, west), (every, ym, low, east), (every, yp, high, east)),
        )[phase]
        along_y, along_z = ((z, yp), (z, ym)), ((zp, y), (zm, y))
        theres = along_y + along_z if phase < 2 else along_z + along_y
        if phase > 0:
            spread_arrived(phase - 1)
        for (bz, by, rows, cols), (tz, ty) in zip(steps, theres):
            part = zall_v.at[core, bz, by, rows, cols]
            copy = pltpu.make_async_remote_copy(
                part, part, za_send.at[0], za_recv.at[phase],
                device_id=((tz * Y + ty) * C + core, x), device_id_type=MESH,
            )
            copy.start()

    spread(0)
    with jax.named_scope("w_weights"):
        await_bytes(inp_v, ld_sem.at[3])
        await_bytes(gu_v, ld_sem.at[4])
    hidden_tile(0)
    hidden_tile(1)
    forward_first()
    with jax.named_scope("w_ogopp"):
        ogopp.wait_recv()
    dispatch(ogopp_v, out2_v)
    scatter(out2_v, 2, 1, recv2_sem, (2, 0))
    forward(1)
    hidden_tile(2)
    spread(1)
    scatter(out2_v, 2, 1, recv2_sem, (1, 3))
    forward(2)
    forward(3)
    await_bytes(dw_v, ld_sem.at[6])

    def give_back(src_ref, dst_ref, which, dzs):
        if 0 in dzs:
            dst_ref[at(sp, CAP), :] = src_ref[at(sp, CAP), :]
        give_rows(src_ref, dst_ref, which, [there for _, there in interleaved(dzs, 1)])

    def give_rows(src_ref, dst_ref, which, theres):
        for there in theres:
            pltpu.make_async_remote_copy(
                src_ref.at[at(there, CAP), :],
                dst_ref.at[at(sp, CAP), :],
                ret_send.at[which],
                ret_recv.at[which],
                device_id=(there, x),
                device_id_type=MESH,
            ).start()

    HALF = GROUP // 2

    def half_plane(zz, h):
        return [
            (zz * Y + 2 * h + lax.rem(y + dy, 2)) * C + lax.rem(core + dc, C)
            for dy in (1, 0)
            for dc in (1, 0)
        ]

    def pieces(k):
        if k < 2:
            return [(k, chunk_rows(ORDER[k]), CHUNK)]
        h = k - 2
        return [
            (2 * k - 2 + i, at(lax.rem(z + dz, Z) * 2 + h, CHUNK // 2), CHUNK // 2)
            for i, dz in enumerate(ORDER[2:])
        ]

    def finish_own(k):
        with jax.named_scope(f"w_part{k}"):
            await_bytes(rp_v.at[:, pl.ds(0, CHUNK), :], pn_recv.at[k])
        for _, rows, _ in pieces(k):
            total = p_v[0, rows, :].astype(F32) + rp_v[0, rows, :].astype(F32) + rp_v[1, rows, :].astype(F32)
            b0_v[rows, :] = total.astype(BF)
        if k < 2:
            give_back(b0_v, ret0_v, 0, (ORDER[k],))
        else:
            lists = [half_plane(lax.rem(z + dz, Z), k - 2) for dz in ORDER[2:]]
            give_rows(b0_v, ret0_v, 0, [there for pair in zip(*lists) for there in pair])

    def rows_pair(ref, halves):
        return jnp.concatenate([ref[rows, :] for _, rows, _ in halves], axis=0)

    def put_pair(ref, halves, value):
        start = 0
        for _, rows, size in halves:
            ref[rows, :] = value[start : start + size, :]
            start += size

    for ks in ((0, 1), (2, 3)):
        halves = [piece for k in ks for piece in pieces(k)]
        part = ks[0] // 2
        with jax.named_scope(f"w_opp{part}"):
            await_bytes(r_v.at[2, pl.ds(0, 2 * CHUNK - (0 if part else CAP)), :], recv2_sem.at[part])
        with jax.named_scope(f"w_x{part}"):
            await_bytes(r_v.at[pl.ds(0, 2), pl.ds(0, 2 * CHUNK), :], x_recv.at[part])
        left = jnp.concatenate([rows_pair(r_v.at[j], halves) for j in range(TP)], axis=1)
        d_hidden = mm(left, dw_v[...], (1, 1))
        if ks[0] == 0:
            spread(2)
        put_pair(dgu_v.at[:, pl.ds(0, HID)], halves, (d_hidden * rows_pair(a_v, halves)).astype(BF))
        put_pair(dgu_v.at[:, pl.ds(HID, HID)], halves, (d_hidden * rows_pair(s_v, halves)).astype(BF))
        for j in (1, 3, 2, 0):
            part = mm(rows_pair(dgu_v, halves), gu_v[j * CH : (j + 1) * CH, :], (1, 1))
            put_pair(p_v.at[j], halves, part.astype(BF))
            if j in (1, 3):
                way = 0 if j == 1 else 1
                for i, rows, _ in halves:
                    copy = pltpu.make_async_remote_copy(
                        p_v.at[j, rows, :],
                        rp_v.at[way, rows, :],
                        pn_send.at[0],
                        pn_recv.at[i if i < 2 else i // 2 + 1],
                        device_id=(sp, xp if j == 1 else xm),
                        device_id_type=MESH,
                    )
                    copy.start()
            if j == 2:
                give_back(p_v.at[2], ret2_v, 1, [ORDER[k] for k in ks])
    finish_own(0)
    finish_own(1)

    slot_scale = 1.0 / math.sqrt(SLOTS)

    def down_tiles(lower, upper):
        def tile(n, carry):
            rows = at(n, 256)
            turned = hid_v[:, rows].T
            for j in range(TP):
                part = mm(turned, r_v[j], (1, 0)) * slot_scale
                down_grad_v[rows, at(lax.rem(x + j, TP), CH)] = part.astype(BF)
            return carry

        lax.fori_loop(lower, upper, tile, 0)

    def gate_tiles(lower, upper):
        def tile(n, carry):
            rows = at(n, 256)
            turned = inp_v[:, rows].T
            rows = at(lax.rem(x + n // 2, TP) * 2 + lax.rem(n, 2), 256)
            gate_grad_v[rows, :] = (mm(turned, dgu_v[:, 0:HID], (1, 0)) * slot_scale).astype(BF)
            up_grad_v[rows, :] = (mm(turned, dgu_v[:, HID : 2 * HID], (1, 0)) * slot_scale).astype(BF)
            return carry

        lax.fori_loop(lower, upper, tile, 0)

    finish_own(2)
    finish_own(3)

    def await_returned(ref, which):
        with jax.named_scope(f"w_ret{which}"):
            await_bytes(ref.at[pl.ds(0, SLOTS - CAP), :], ret_recv.at[which])

    def to_opposite(src, dst, send_sem, recv_sem):
        copy = pltpu.make_async_remote_copy(
            src, dst, send_sem, recv_sem, device_id=(sp, xo), device_id_type=MESH
        )
        copy.start()
        return copy

    await_returned(ret2_v, 1)
    m2_v[...] = mm(disp_v[...], ret2_v[...], (0, 0)).astype(BF)
    m2 = to_opposite(m2_v, r2_v, m2_sem.at[0], m2_sem.at[1])
    spread(3)
    with jax.named_scope("g_gate"):
        gate_tiles(0, 4)
    await_returned(ret0_v, 0)
    moe = mm(disp_v[...], ret0_v[...], (0, 0))
    m0_v[...] = moe.astype(BF)

    def lanes(s):
        return at(lax.rem(y + s, Y), TOK)

    def send_m0(s):
        to_opposite(m0_v.at[:, lanes(s)], rm0_v.at[:, lanes(s)], m0_sem.at[0], rf_recv.at[s])

    send_m0(2)
    send_m0(0)
    with jax.named_scope("w_m2"):
        m2.wait_recv()
    own = (og_v[...].astype(F32) + moe + r2_v[...].astype(F32)).astype(BF)
    rf_v[0] = own
    def send_rf(s):
        for there, landing in ((xp, 3), (xm, 1)):
            copy = pltpu.make_async_remote_copy(
                rf_v.at[0, :, lanes(s)],
                rf_v.at[landing, :, lanes(s)],
                rf_send.at[0],
                rf_recv.at[s],
                device_id=(sp, there),
                device_id_type=MESH,
            )
            copy.start()

    send_rf(2)
    send_rf(0)
    send_m0(1)
    send_m0(3)
    send_rf(1)
    send_rf(3)
    resid_v[...] = own
    loads[9].wait()

    def mix_part(j):
        return mm(rf_v[j], pw_v[at(lax.rem(x + j, TP), CH), :], (1, 0))

    def order_of(cc, zz, yy):
        return (cc * Z + zz) * Y + yy

    mine = order_of(core, z, y)

    def share(j, s):
        block = lax.rem(x + j, TP)
        across = lax.rem(y + s, Y)
        rft_v[j, across] = rf_v[j, :, lanes(s)].T.reshape(C, ROWS, TOK)
        for dc in (1, 0):
            inside = lax.rem(core + dc, C)
            there = (block * Y + across) * C + inside

            @pl.when(there != sp)
            def _():
                pltpu.make_async_remote_copy(
                    rft_v.at[j, across, inside],
                    rt_v.at[mine],
                    rt_send.at[0],
                    rt_recv.at[lax.rem(z - block + Z, Z)],
                    device_id=(there, x),
                    device_id_type=MESH,
                ).start()

    for s in (2, 0, 1, 3):
        share(0, s)
    mix = mix_part(0)
    with jax.named_scope("g_gate2"):
        gate_tiles(4, 8)
    for s in (2, 0, 1, 3):
        with jax.named_scope(f"w_rf_{s}"):
            await_bytes(rf_v.at[pl.ds(0, 3), :, pl.ds(0, TOK)], rf_recv.at[s])
        share(3, s)
        share(1, s)
        cols = lanes(s)
        other = ogopp_v[:, cols].astype(F32) + rm0_v[:, cols].astype(F32) + m2_v[:, cols].astype(F32)
        rf_v[2, :, cols] = other.astype(BF)
        share(2, s)
        if s == 2:
            spread_arrived(3)
            to_partner = pltpu.make_async_remote_copy(
                zall_v.at[core], zall_v.at[core], zd_sem.at[0], zd_sem.at[1],
                device_id=(partner, x), device_id_type=MESH,
            )
            to_partner.start()
    for j in (3, 1, 2):
        mix = mix + mix_part(j)
    ogg_v[...] = (mix * conv_vals).astype(BF)
    cg_v[...] = (mix * gate_vals).astype(BF)
    down = pltpu.make_async_remote_copy(
        cg_v.at[pl.ds(0, 16), :], after_v, halo_sem.at[0], halo_sem.at[1],
        device_id=(lax.rem(sp + SP - 1, SP), x), device_id_type=MESH,
    )
    up = pltpu.make_async_remote_copy(
        cg_v.at[pl.ds(TOK - 16, 16), :], before_v, halo_sem.at[0], halo_sem.at[1],
        device_id=(lax.rem(sp + 1, SP), x), device_id_type=MESH,
    )
    down.start()
    up.start()
    rt_v[mine] = rft_v[lax.rem(z - x + TP, TP), y, core]
    with jax.named_scope("g_down"):
        down_tiles(0, HID // 256)
    ogopp.wait_send()
    for which, ref in ((0, out0_v), (1, out2_v)):
        await_bytes(ref.at[pl.ds(0, SLOTS - CAP), :], disp_sem.at[which])
        await_bytes(ref.at[pl.ds(0, SLOTS - CAP), :], ret_send.at[which])
    m2.wait_send()
    await_bytes(r_v.at[pl.ds(0, 2)], x_send.at[0])
    await_bytes(r_v.at[pl.ds(0, 2)], pn_send.at[0])
    with jax.named_scope("w_zd"):
        to_partner.wait_recv()

    def proj_group(dz):
        count = GROUP - 1 if dz == 0 else GROUP
        with jax.named_scope(f"w_rt{dz}"):
            await_bytes(rt_v.at[pl.ds(0, count)], rt_recv.at[dz])
        zz = lax.rem(z + dz, Z)
        total = None
        for cc in range(C):
            left = jnp.concatenate([rt_v[order_of(cc, zz, yy)] for yy in range(Y)], axis=1)
            term = mm(left, zall_v[cc, zz].reshape(Y * TOK, CH), (1, 0))
            total = term if total is None else total + term
        return total

    proj = proj_group(0) + proj_group(1)

    loads[12].wait()
    with jax.named_scope("w_halo"):
        await_bytes(cg_v.at[pl.ds(0, 32), :], halo_sem.at[1])
    cg = cg_v[...].astype(F32)
    taps = taps_v[...].astype(F32)
    row = lax.broadcasted_iota(jnp.int32, (TOK, CH), 0)
    has_before = jnp.where(sp > 0, 1.0, 0.0)
    has_after = jnp.where(sp < SP - 1, 1.0, 0.0)
    before = before_v[...].astype(F32)[15:16, :] * has_before
    after = after_v[...].astype(F32)[0:1, :] * has_after
    nxt = jnp.where(row == TOK - 1, jnp.broadcast_to(after, (TOK, CH)), pltpu.roll(cg, TOK - 1, 0))
    prv = jnp.where(row == 0, jnp.broadcast_to(before, (TOK, CH)), pltpu.roll(cg, 1, 0))
    value_grad = nxt * taps[0:1, :] + cg * taps[1:2, :] + prv * taps[2:3, :]
    igg_v[...] = (value_grad * val_v[...].astype(F32)).astype(BF)
    vg_v[...] = (value_grad * ing_v[...].astype(F32)).astype(BF)

    proj = proj + proj_group(3)
    proj = proj + proj_group(2)
    proj_v[...] = proj * (1.0 / math.sqrt(TOK * SP))

    await_bytes(r_v.at[:, pl.ds(0, 15 * TOK // TP), :], za_send.at[0])
    to_partner.wait_send()
    await_bytes(m0_v, m0_sem.at[0])
    await_bytes(rf_v.at[pl.ds(0, 2)], rf_send.at[0])
    await_bytes(cg_v.at[pl.ds(0, 32), :], halo_sem.at[0])
    await_bytes(rt_v.at[pl.ds(0, SP - 1)], rt_send.at[0])


def flush_kernel(*refs):
    count = (len(refs) - 1) // 2
    sems = refs[-1]
    for i in reversed(range(count)):
        src, dst = refs[i], refs[count + i]
        pieces = 4 if i >= count - 3 else 1
        rows = src.shape[0] // pieces
        for p in range(pieces):
            part = pl.ds(p * rows, rows)
            pltpu.make_async_copy(src.at[part, :], dst.at[part, :], sems.at[i]).start()
    for i in range(count):
        pltpu.make_async_copy(refs[i], refs[count + i], sems.at[i]).wait()


def per_device(
    out_grad, route_ids, route_weight, expert_inputs, gate_weight, up_weight, down_weight,
    out_gate, in_gate, values, conv_out, conv_taps, proj_weight,
):
    sds = jax.ShapeDtypeStruct
    hbm = pl.BlockSpec(memory_space=pltpu.HBM)
    vm = pltpu.VMEM
    dma = pltpu.SemaphoreType.DMA
    act = (TOK, CH)
    vmem = pl.BlockSpec(memory_space=pltpu.VMEM)
    shapes = [
        sds(act, BF), sds(act, BF), sds(act, BF), sds(act, BF), sds((ROWS, CH), F32),
        sds((TP * CH, HID), BF), sds((TP * CH, HID), BF), sds((HID, TP * CH), BF),
    ]
    outs = pl.pallas_call(
        layer_kernel,
        in_specs=[hbm] * 13,
        out_specs=[vmem] * 8,
        out_shape=[vm(o.shape, o.dtype) for o in shapes],
        scratch_shapes=[
            vm((2, TOK), jnp.int32), vm((2, TOK), F32), vm(act, BF), vm((SLOTS, TP * CH), BF),
            vm((TP * CH, 2 * HID), BF), vm((HID, TP * CH), BF), vm(act, BF), vm(act, BF), vm(act, BF),
            vm(act, BF), vm((3, CH), BF), vm((TP * CH, CH), BF),
            vm(act, BF), vm((SLOTS, TOK), BF), vm((SLOTS, TOK), F32), vm((SLOTS, CH), BF),
            vm((SLOTS, CH), BF), vm((TP, SLOTS, CH), BF), vm((SLOTS, HID), F32), vm((SLOTS, HID), F32),
            vm((SLOTS, HID), BF), vm((SLOTS, 2 * HID), BF),
            vm((TP, SLOTS, CH), BF), vm((2, SLOTS, CH), BF), vm((SLOTS, CH), BF), vm((SLOTS, CH), BF),
            vm((SLOTS, CH), BF), vm(act, BF), vm(act, BF), vm(act, BF), vm(act, BF),
            vm((TP,) + act, BF), vm(act, BF), vm((16, CH), BF), vm((16, CH), BF),
            vm((C, Z, Y) + act, BF), vm((TP, Y, C, ROWS, TOK), BF), vm((SP, ROWS, TOK), BF),
            dma((9,)), dma((2,)), dma((2,)), dma((Z + 1,)), dma((2,)), dma((1,)), dma((2,)),
            dma((1,)), dma((Z,)), dma((2,)), dma((2,)), dma((2,)), dma((1,)), dma((1,)), dma((Y,)),
            dma((2,)), dma((1,)), dma((4,)), dma((2,)), dma((1,)), dma((Z,)),
        ],
        compiler_params=pltpu.CompilerParams(
            collective_id=0, has_side_effects=True, vmem_limit_bytes=52428800
        ),
    )(
        route_ids.T, route_weight.T, out_grad, expert_inputs[0], gate_weight[0], up_weight[0],
        down_weight[0], out_gate, in_gate, values, conv_out, conv_taps, proj_weight,
    )
    resid, ogg, igg, vg, proj, gate_grad, up_grad, down_grad = pl.pallas_call(
        flush_kernel,
        in_specs=[vmem] * 8,
        out_specs=[hbm] * 8,
        out_shape=shapes,
        scratch_shapes=[dma((8,))],
        compiler_params=pltpu.CompilerParams(vmem_limit_bytes=1024 * 1024),
    )(*outs)
    return resid, ogg, igg, vg, proj, gate_grad[None], up_grad[None], down_grad[None]


def solution(mesh):
    return jax.shard_map(
        per_device,
        mesh=mesh,
        in_specs=(
            P("sp", "tp"), P("sp", None), P("sp", None), P("sp", None, None), P("sp", None, "tp"),
            P("sp", None, "tp"), P("sp", "tp", None), P("sp", "tp"), P("sp", "tp"), P("sp", "tp"),
            P("sp", "tp"), P(None, "tp"), P(None, "tp"),
        ),
        out_specs=(
            P("sp", "tp"), P("sp", "tp"), P("sp", "tp"), P("sp", "tp"), P("sp", "tp"),
            P("sp", None, "tp"), P("sp", None, "tp"), P("sp", "tp", None),
        ),
        check_vma=False,
    )
```

```python
import functools
import math

import jax
import jax.numpy as jnp
from jax import lax
from jax.experimental import pallas as pl
from jax.experimental.pallas import tpu as pltpu
from jax.sharding import PartitionSpec as P

MESH = pl.DeviceIdType.MESH
BF = jnp.bfloat16
F32 = jnp.float32

Z, Y, C = 4, 4, 2
SP = Z * Y * C
TP = 4
TOK = 128
CAP = 16
SLOTS = SP * CAP
CH = 512
HID = 768
ROWS = 64
GROUP = Y * C
CHUNK = GROUP * CAP
ORDER = (0, 2, 1, 3)
FAR_FIRST = (2, 1, 3, 0)


def mm(a, b, dims):
    return lax.dot_general(a, b, ((dims[:1], dims[1:]), ((), ())), preferred_element_type=F32)


def at(block, size):
    return pl.ds(pl.multiple_of(block * size, size), size)


def layer_kernel(
    ids_hbm, w_hbm, og_hbm, inp_hbm, gw_hbm, uw_hbm, dw_hbm,
    gate_hbm, ing_hbm, val_hbm, conv_hbm, taps_hbm, pw_hbm,
    resid_v, ogg_v, igg_v, vg_v, proj_v, gate_grad_v, up_grad_v, down_grad_v,
    ids_v, w_v, og_v, inp_v, gu_v, dw_v, gate_v, ing_v, val_v, conv_v, taps_v, pw_v,
    ogopp_v, disp_v, wslot_v, out0_v, out2_v, r_v, s_v, a_v, hid_v, dgu_v,
    p_v, rp_v, b0_v, ret0_v, ret2_v, m2_v, r2_v, m0_v, rm0_v, rf_v, cg_v, before_v, after_v,
    zall_v, rft_v, rt_v,
    ld_sem, ogopp_sem, disp_sem, recv0_sem, recv2_sem, x_send, x_recv,
    pn_send, pn_recv, ret_send, ret_recv, m2_sem, m0_sem, rf_send, rf_recv, halo_sem, za_send, za_recv,
    zd_sem, rt_send, rt_recv,
):
    sp = lax.axis_index("sp")
    x = lax.axis_index("tp")
    z = sp // GROUP
    inner = lax.rem(sp, GROUP)
    core = lax.rem(sp, C)
    chip = sp // C
    y = lax.rem(chip, Y)
    xp, xm, xo = lax.rem(x + 1, TP), lax.rem(x + 3, TP), lax.rem(x + 2, TP)

    def load(i, src, dst):
        copy = pltpu.make_async_copy(src, dst, ld_sem.at[i])
        copy.start()
        return copy

    first_loads = {
        0: load(0, ids_hbm, ids_v),
        1: load(1, w_hbm, w_v),
        2: load(2, og_hbm, og_v),
    }
    barrier = pltpu.get_barrier_semaphore()

    def greet(s, t):
        pl.semaphore_signal(barrier, inc=1, device_id=(s, t), device_id_type=MESH)

    for dz in FAR_FIRST:
        for dy in FAR_FIRST:
            for dc in (1, 0):
                if dz or dy or dc:
                    chip_there = lax.rem(z + dz, Z) * Y + lax.rem(y + dy, Y)
                    greet(chip_there * C + lax.rem(core + dc, C), x)
        if dz == 2:
            for t in (xo, xp, xm):
                greet(sp, t)

    def blocks(i, pairs):
        for j in range(TP):
            for src, dst in pairs(at(lax.rem(x + j, TP), CH), pl.ds(j * CH, CH)):
                load(i, src, dst)

    loads = first_loads
    load(7, gate_hbm, gate_v)
    load(7, conv_hbm, conv_v)
    load(7, ing_hbm, ing_v)
    load(7, val_hbm, val_v)
    blocks(3, lambda theirs, ours: [(inp_hbm.at[:, theirs], inp_v.at[:, ours])])
    blocks(4, lambda theirs, ours: [
        (gw_hbm.at[theirs, :], gu_v.at[ours, pl.ds(0, HID)]),
        (uw_hbm.at[theirs, :], gu_v.at[ours, pl.ds(HID, HID)]),
    ])
    blocks(6, lambda theirs, ours: [(dw_hbm.at[:, theirs], dw_v.at[:, ours])])
    loads |= {
        9: load(5, pw_hbm, pw_v),
        12: load(8, taps_hbm, taps_v),
    }

    def await_bytes(ref, sem):
        pltpu.make_async_copy(ref, ref, sem).wait()


    with jax.named_scope("w_load"):
        loads[0].wait()
        loads[1].wait()
        loads[2].wait()
    ids = ids_v[...]
    wts = w_v[...]
    e_iota = lax.broadcasted_iota(jnp.int32, (SP, TOK), 0)
    first = e_iota == ids[0:1, :]
    second = e_iota == ids[1:2, :]
    named = jnp.where(first | second, 1.0, 0.0)
    w_et = jnp.where(first, wts[0:1, :], 0.0) + jnp.where(second, wts[1:2, :], 0.0)
    earlier = lax.broadcasted_iota(jnp.int32, (TOK, TOK), 0) < lax.broadcasted_iota(
        jnp.int32, (TOK, TOK), 1
    )
    prefix = mm(named.astype(BF), jnp.where(earlier, 1.0, 0.0).astype(BF), (1, 0))
    rank = jnp.where(named > 0.5, prefix, -1.0)
    r_iota = lax.broadcasted_iota(jnp.int32, (SP, CAP, TOK), 1).astype(F32)
    hit = jnp.broadcast_to(rank[:, None, :], (SP, CAP, TOK)) == r_iota
    disp = jnp.where(hit, 1.0, 0.0)
    wslot = jnp.sum(disp * w_et[:, None, :], axis=2, keepdims=True)
    disp_v[...] = disp.reshape(SLOTS, TOK).astype(BF)
    wslot_v[...] = jnp.broadcast_to(wslot, (SP, CAP, TOK)).reshape(SLOTS, TOK)

    def dispatch(tok_ref, out_ref):
        rows = mm(disp_v[...], tok_ref[...], (1, 0))
        out_ref[...] = (rows * jnp.tile(wslot_v[...], (1, CH // TOK))).astype(BF)

    dispatch(og_v, out0_v)
    TILE = 256

    def hidden_tile(n):
        cols = slice(n * TILE, (n + 1) * TILE)
        ups = slice(HID + n * TILE, HID + (n + 1) * TILE)

        def rows_of(m, carry):
            rows = at(m, 256)
            pre_gate = mm(inp_v[rows, :], gu_v[:, cols], (1, 0))
            pre_up = mm(inp_v[rows, :], gu_v[:, ups], (1, 0))
            sig = 1.0 / (1.0 + jnp.exp(-pre_gate))
            act = pre_gate * sig
            s_v[rows, cols] = act
            a_v[rows, cols] = pre_up * sig * (1.0 + pre_gate * (1.0 - sig))
            hid_v[rows, cols] = (act * pre_up).astype(BF)
            return carry

        lax.fori_loop(0, SLOTS // 256, rows_of, 0)

    with jax.named_scope("w_barrier"):
        pl.semaphore_wait(barrier, SP - 1 + TP - 1)

    ogopp = pltpu.make_async_remote_copy(
        og_v, ogopp_v, ogopp_sem.at[0], ogopp_sem.at[1], device_id=(sp, xo), device_id_type=MESH
    )
    ogopp.start()

    def plane(zz, skip_self):
        peers = []
        for dy in FAR_FIRST:
            for dc in (1, 0):
                if not (skip_self and dy == 0 and dc == 0):
                    peers.append((zz * Y + lax.rem(y + dy, Y)) * C + lax.rem(core + dc, C))
        return peers

    def interleaved(dzs, sign):
        lists = [[(dz, there) for there in plane(lax.rem(z + sign * dz + Z, Z), dz == 0)] for dz in dzs]
        return [entry for i in range(GROUP) for entries in lists for entry in entries[i : i + 1]]

    def scatter(out_ref, block, which, recv_sem, dzs):
        if 0 in dzs:
            r_v[block, at(sp, CAP), :] = out_ref[at(sp, CAP), :]
        for dz, there in interleaved(dzs, -1):
            pltpu.make_async_remote_copy(
                out_ref.at[at(there, CAP), :],
                r_v.at[block, at(sp, CAP), :],
                disp_sem.at[which],
                recv_sem.at[dz % 2 if block == 2 else dz],
                device_id=(there, x),
                device_id_type=MESH,
            ).start()

    def chunk_rows(dz):
        return at(lax.rem(z + dz, Z), CHUNK)

    r_v[0, at(sp, CAP), :] = out0_v[at(sp, CAP), :]
    for dy in (1, 3, 0, 2):
        for dc in (1, 0) if dy else (1,):
            there = (z * Y + lax.rem(y + dy, Y)) * C + lax.rem(core + dc, C)
            pltpu.make_async_remote_copy(
                out0_v.at[at(there, CAP), :],
                r_v.at[0, at(sp, CAP), :],
                disp_sem.at[0],
                recv0_sem.at[Z if dy == 2 else 0],
                device_id=(there, x),
                device_id_type=MESH,
            ).start()
    scatter(out0_v, 0, 0, recv0_sem, (2,))
    scatter(out0_v, 0, 0, recv0_sem, (1, 3))

    def await_group(block, dz, recv_sem):
        count = CHUNK - CAP if dz == 0 else CHUNK
        with jax.named_scope(f"w_group{block}_{dz}"):
            await_bytes(r_v.at[block, pl.ds(0, count), :], recv_sem.at[dz])

    def forward_rows(k, rows):
        for way, (there, landing) in enumerate(((xp, 3), (xm, 1))):
            copy = pltpu.make_async_remote_copy(
                r_v.at[0, rows, :],
                r_v.at[landing, rows, :],
                x_send.at[0],
                x_recv.at[k // 2],
                device_id=(sp, there),
                device_id_type=MESH,
            )
            copy.start()

    def forward_first():
        near = C * CAP
        with jax.named_scope("w_group0_0"):
            await_bytes(r_v.at[0, pl.ds(0, 3 * near - CAP), :], recv0_sem.at[0])
        for dy in (0, 1, 3):
            forward_rows(0, at(z * Y + lax.rem(y + dy, Y), near))
        with jax.named_scope("w_group0_far"):
            await_bytes(r_v.at[0, pl.ds(0, near), :], recv0_sem.at[Z])
        forward_rows(0, at(z * Y + lax.rem(y + 2, Y), near))

    def forward(k):
        await_group(0, ORDER[k], recv0_sem)
        forward_rows(k, chunk_rows(ORDER[k]))

    await_bytes(rf_v, ld_sem.at[7])
    gate_vals = gate_v[...].astype(F32)
    conv_vals = conv_v[...].astype(F32)
    zall_v[core, z, y] = (gate_vals * conv_vals).astype(BF)
    partner = sp + 1 - 2 * core
    zp, zm = lax.rem(z + 1, Z), lax.rem(z + 3, Z)
    yp, ym = lax.rem(y + 1, Y), lax.rem(y + 3, Y)
    west, east = pl.ds(0, CH // 2), pl.ds(CH // 2, CH // 2)
    low, high, full = pl.ds(0, TOK // 2), pl.ds(TOK // 2, TOK // 2), pl.ds(0, TOK)
    every = pl.ds(0, Z)

    def spread_arrived(phase):
        rows = (2 * TOK, TOK, 8 * TOK, 4 * TOK)[phase]
        with jax.named_scope(f"w_spread{phase + 1}"):
            await_bytes(r_v.at[pl.ds(0, rows // TOK), pl.ds(0, TOK), :] if rows <= 2 * TOK else r_v.at[pl.ds(0, 2), pl.ds(0, rows // 2), :], za_recv.at[phase])

    def spread(phase):
        steps = (
            ((z, y, full, west), (z, y, full, west), (z, y, full, east), (z, y, full, east)),
            ((z, ym, low, west), (z, yp, high, west), (zm, y, low, east), (zp, y, high, east)),
            ((z, every, full, west), (z, every, full, west), (every, y, full, east), (every, y, full, east)),
            ((zm, every, low, west), (zp, every, high, west), (every, ym, low, east), (every, yp, high, east)),
        )[phase]
        along_y, along_z = ((z, yp), (z, ym)), ((zp, y), (zm, y))
        theres = along_y + along_z if phase < 2 else along_z + along_y
        if phase > 0:
            spread_arrived(phase - 1)
        for (bz, by, rows, cols), (tz, ty) in zip(steps, theres):
            part = zall_v.at[core, bz, by, rows, cols]
            copy = pltpu.make_async_remote_copy(
                part, part, za_send.at[0], za_recv.at[phase],
                device_id=((tz * Y + ty) * C + core, x), device_id_type=MESH,
            )
            copy.start()

    spread(0)
    with jax.named_scope("w_weights"):
        await_bytes(inp_v, ld_sem.at[3])
        await_bytes(gu_v, ld_sem.at[4])
    hidden_tile(0)
    hidden_tile(1)
    forward_first()
    with jax.named_scope("w_ogopp"):
        ogopp.wait_recv()
    dispatch(ogopp_v, out2_v)
    scatter(out2_v, 2, 1, recv2_sem, (2, 0))
    forward(1)
    hidden_tile(2)
    forward(2)
    forward(3)
    spread(1)
    scatter(out2_v, 2, 1, recv2_sem, (1, 3))
    await_bytes(dw_v, ld_sem.at[6])

    def give_back(src_ref, dst_ref, which, dzs):
        if 0 in dzs:
            dst_ref[at(sp, CAP), :] = src_ref[at(sp, CAP), :]
        give_rows(src_ref, dst_ref, which, [there for _, there in interleaved(dzs, 1)])

    def give_rows(src_ref, dst_ref, which, theres):
        for there in theres:
            pltpu.make_async_remote_copy(
                src_ref.at[at(there, CAP), :],
                dst_ref.at[at(sp, CAP), :],
                ret_send.at[which],
                ret_recv.at[which],
                device_id=(there, x),
                device_id_type=MESH,
            ).start()

    HALF = GROUP // 2

    def half_plane(zz, h):
        return [
            (zz * Y + 2 * h + lax.rem(y + dy, 2)) * C + lax.rem(core + dc, C)
            for dy in (1, 0)
            for dc in (1, 0)
        ]

    def pieces(k):
        if k < 2:
            return [(k, chunk_rows(ORDER[k]), CHUNK)]
        h = k - 2
        return [
            (2 * k - 2 + i, at(lax.rem(z + dz, Z) * 2 + h, CHUNK // 2), CHUNK // 2)
            for i, dz in enumerate(ORDER[2:])
        ]

    def finish_own(k):
        with jax.named_scope(f"w_part{k}"):
            await_bytes(rp_v.at[:, pl.ds(0, CHUNK), :], pn_recv.at[k])
        for _, rows, _ in pieces(k):
            total = p_v[0, rows, :].astype(F32) + rp_v[0, rows, :].astype(F32) + rp_v[1, rows, :].astype(F32)
            b0_v[rows, :] = total.astype(BF)
        if k < 2:
            give_back(b0_v, ret0_v, 0, (ORDER[k],))
        else:
            lists = [half_plane(lax.rem(z + dz, Z), k - 2) for dz in ORDER[2:]]
            give_rows(b0_v, ret0_v, 0, [there for pair in zip(*lists) for there in pair])

    def rows_pair(ref, halves):
        return jnp.concatenate([ref[rows, :] for _, rows, _ in halves], axis=0)

    def put_pair(ref, halves, value):
        start = 0
        for _, rows, size in halves:
            ref[rows, :] = value[start : start + size, :]
            start += size

    for ks in ((0, 1), (2, 3)):
        halves = [piece for k in ks for piece in pieces(k)]
        part = ks[0] // 2
        with jax.named_scope(f"w_opp{part}"):
            await_bytes(r_v.at[2, pl.ds(0, 2 * CHUNK - (0 if part else CAP)), :], recv2_sem.at[part])
        with jax.named_scope(f"w_x{part}"):
            await_bytes(r_v.at[pl.ds(0, 2), pl.ds(0, 2 * CHUNK), :], x_recv.at[part])
        left = jnp.concatenate([rows_pair(r_v.at[j], halves) for j in range(TP)], axis=1)
        d_hidden = mm(left, dw_v[...], (1, 1))
        if ks[0] == 0:
            spread(2)
        put_pair(dgu_v.at[:, pl.ds(0, HID)], halves, (d_hidden * rows_pair(a_v, halves)).astype(BF))
        put_pair(dgu_v.at[:, pl.ds(HID, HID)], halves, (d_hidden * rows_pair(s_v, halves)).astype(BF))
        for j in (1, 3, 2, 0):
            part = mm(rows_pair(dgu_v, halves), gu_v[j * CH : (j + 1) * CH, :], (1, 1))
            put_pair(p_v.at[j], halves, part.astype(BF))
            if j in (1, 3):
                way = 0 if j == 1 else 1
                for i, rows, _ in halves:
                    copy = pltpu.make_async_remote_copy(
                        p_v.at[j, rows, :],
                        rp_v.at[way, rows, :],
                        pn_send.at[0],
                        pn_recv.at[i if i < 2 else i // 2 + 1],
                        device_id=(sp, xp if j == 1 else xm),
                        device_id_type=MESH,
                    )
                    copy.start()
            if j == 2:
                give_back(p_v.at[2], ret2_v, 1, [ORDER[k] for k in ks])
    finish_own(0)
    finish_own(1)

    slot_scale = 1.0 / math.sqrt(SLOTS)

    def down_tiles(lower, upper):
        def tile(n, carry):
            rows = at(n, 256)
            turned = hid_v[:, rows].T
            for j in range(TP):
                part = mm(turned, r_v[j], (1, 0)) * slot_scale
                down_grad_v[rows, at(lax.rem(x + j, TP), CH)] = part.astype(BF)
            return carry

        lax.fori_loop(lower, upper, tile, 0)

    def gate_tiles(lower, upper):
        def tile(n, carry):
            rows = at(n, 256)
            turned = inp_v[:, rows].T
            rows = at(lax.rem(x + n // 2, TP) * 2 + lax.rem(n, 2), 256)
            gate_grad_v[rows, :] = (mm(turned, dgu_v[:, 0:HID], (1, 0)) * slot_scale).astype(BF)
            up_grad_v[rows, :] = (mm(turned, dgu_v[:, HID : 2 * HID], (1, 0)) * slot_scale).astype(BF)
            return carry

        lax.fori_loop(lower, upper, tile, 0)

    finish_own(2)
    finish_own(3)

    def await_returned(ref, which):
        with jax.named_scope(f"w_ret{which}"):
            await_bytes(ref.at[pl.ds(0, SLOTS - CAP), :], ret_recv.at[which])

    def to_opposite(src, dst, send_sem, recv_sem):
        copy = pltpu.make_async_remote_copy(
            src, dst, send_sem, recv_sem, device_id=(sp, xo), device_id_type=MESH
        )
        copy.start()
        return copy

    await_returned(ret2_v, 1)
    m2_v[...] = mm(disp_v[...], ret2_v[...], (0, 0)).astype(BF)
    m2 = to_opposite(m2_v, r2_v, m2_sem.at[0], m2_sem.at[1])
    spread(3)
    with jax.named_scope("g_gate"):
        gate_tiles(0, 4)
    await_returned(ret0_v, 0)
    moe = mm(disp_v[...], ret0_v[...], (0, 0))
    m0_v[...] = moe.astype(BF)

    def lanes(s):
        return at(lax.rem(y + s, Y), TOK)

    def send_m0(s):
        to_opposite(m0_v.at[:, lanes(s)], rm0_v.at[:, lanes(s)], m0_sem.at[0], rf_recv.at[s])

    send_m0(2)
    send_m0(0)
    with jax.named_scope("w_m2"):
        m2.wait_recv()
    own = (og_v[...].astype(F32) + moe + r2_v[...].astype(F32)).astype(BF)
    rf_v[0] = own
    def send_rf(s):
        for there, landing in ((xp, 3), (xm, 1)):
            copy = pltpu.make_async_remote_copy(
                rf_v.at[0, :, lanes(s)],
                rf_v.at[landing, :, lanes(s)],
                rf_send.at[0],
                rf_recv.at[s],
                device_id=(sp, there),
                device_id_type=MESH,
            )
            copy.start()

    send_rf(2)
    send_rf(0)
    send_m0(1)
    send_m0(3)
    send_rf(1)
    send_rf(3)
    resid_v[...] = own
    loads[9].wait()

    def mix_part(j):
        return mm(rf_v[j], pw_v[at(lax.rem(x + j, TP), CH), :], (1, 0))

    def order_of(cc, zz, yy):
        return (cc * Z + zz) * Y + yy

    mine = order_of(core, z, y)

    def share(j, s):
        block = lax.rem(x + j, TP)
        across = lax.rem(y + s, Y)
        rft_v[j, across] = rf_v[j, :, lanes(s)].T.reshape(C, ROWS, TOK)
        for dc in (1, 0):
            inside = lax.rem(core + dc, C)
            there = (block * Y + across) * C + inside

            @pl.when(there != sp)
            def _():
                pltpu.make_async_remote_copy(
                    rft_v.at[j, across, inside],
                    rt_v.at[mine],
                    rt_send.at[0],
                    rt_recv.at[lax.rem(z - block + Z, Z)],
                    device_id=(there, x),
                    device_id_type=MESH,
                ).start()

    for s in (2, 0, 1, 3):
        share(0, s)
    mix = mix_part(0)
    with jax.named_scope("g_gate2"):
        gate_tiles(4, 8)
    for s in (2, 0, 1, 3):
        with jax.named_scope(f"w_rf_{s}"):
            await_bytes(rf_v.at[pl.ds(0, 3), :, pl.ds(0, TOK)], rf_recv.at[s])
        share(3, s)
        share(1, s)
        cols = lanes(s)
        other = ogopp_v[:, cols].astype(F32) + rm0_v[:, cols].astype(F32) + m2_v[:, cols].astype(F32)
        rf_v[2, :, cols] = other.astype(BF)
        share(2, s)
        if s == 2:
            spread_arrived(3)
            to_partner = pltpu.make_async_remote_copy(
                zall_v.at[core], zall_v.at[core], zd_sem.at[0], zd_sem.at[1],
                device_id=(partner, x), device_id_type=MESH,
            )
            to_partner.start()
    for j in (3, 1, 2):
        mix = mix + mix_part(j)
    ogg_v[...] = (mix * conv_vals).astype(BF)
    cg_v[...] = (mix * gate_vals).astype(BF)
    down = pltpu.make_async_remote_copy(
        cg_v.at[pl.ds(0, 16), :], after_v, halo_sem.at[0], halo_sem.at[1],
        device_id=(lax.rem(sp + SP - 1, SP), x), device_id_type=MESH,
    )
    up = pltpu.make_async_remote_copy(
        cg_v.at[pl.ds(TOK - 16, 16), :], before_v, halo_sem.at[0], halo_sem.at[1],
        device_id=(lax.rem(sp + 1, SP), x), device_id_type=MESH,
    )
    down.start()
    up.start()
    rt_v[mine] = rft_v[lax.rem(z - x + TP, TP), y, core]
    with jax.named_scope("g_down"):
        down_tiles(0, HID // 256)
    ogopp.wait_send()
    for which, ref in ((0, out0_v), (1, out2_v)):
        await_bytes(ref.at[pl.ds(0, SLOTS - CAP), :], disp_sem.at[which])
        await_bytes(ref.at[pl.ds(0, SLOTS - CAP), :], ret_send.at[which])
    m2.wait_send()
    await_bytes(r_v.at[pl.ds(0, 2)], x_send.at[0])
    await_bytes(r_v.at[pl.ds(0, 2)], pn_send.at[0])
    with jax.named_scope("w_zd"):
        to_partner.wait_recv()

    def proj_group(dz):
        count = GROUP - 1 if dz == 0 else GROUP
        with jax.named_scope(f"w_rt{dz}"):
            await_bytes(rt_v.at[pl.ds(0, count)], rt_recv.at[dz])
        zz = lax.rem(z + dz, Z)
        total = None
        for cc in range(C):
            left = jnp.concatenate([rt_v[order_of(cc, zz, yy)] for yy in range(Y)], axis=1)
            term = mm(left, zall_v[cc, zz].reshape(Y * TOK, CH), (1, 0))
            total = term if total is None else total + term
        return total

    proj = proj_group(0) + proj_group(1)

    loads[12].wait()
    with jax.named_scope("w_halo"):
        await_bytes(cg_v.at[pl.ds(0, 32), :], halo_sem.at[1])
    cg = cg_v[...].astype(F32)
    taps = taps_v[...].astype(F32)
    row = lax.broadcasted_iota(jnp.int32, (TOK, CH), 0)
    has_before = jnp.where(sp > 0, 1.0, 0.0)
    has_after = jnp.where(sp < SP - 1, 1.0, 0.0)
    before = before_v[...].astype(F32)[15:16, :] * has_before
    after = after_v[...].astype(F32)[0:1, :] * has_after
    nxt = jnp.where(row == TOK - 1, jnp.broadcast_to(after, (TOK, CH)), pltpu.roll(cg, TOK - 1, 0))
    prv = jnp.where(row == 0, jnp.broadcast_to(before, (TOK, CH)), pltpu.roll(cg, 1, 0))
    value_grad = nxt * taps[0:1, :] + cg * taps[1:2, :] + prv * taps[2:3, :]
    igg_v[...] = (value_grad * val_v[...].astype(F32)).astype(BF)
    vg_v[...] = (value_grad * ing_v[...].astype(F32)).astype(BF)

    proj = proj + proj_group(3)
    proj = proj + proj_group(2)
    proj_v[...] = proj * (1.0 / math.sqrt(TOK * SP))

    await_bytes(r_v.at[:, pl.ds(0, 15 * TOK // TP), :], za_send.at[0])
    to_partner.wait_send()
    await_bytes(m0_v, m0_sem.at[0])
    await_bytes(rf_v.at[pl.ds(0, 2)], rf_send.at[0])
    await_bytes(cg_v.at[pl.ds(0, 32), :], halo_sem.at[0])
    await_bytes(rt_v.at[pl.ds(0, SP - 1)], rt_send.at[0])


def flush_kernel(*refs):
    count = (len(refs) - 1) // 2
    sems = refs[-1]
    for i in reversed(range(count)):
        src, dst = refs[i], refs[count + i]
        pieces = 4 if i >= count - 3 else 1
        rows = src.shape[0] // pieces
        for p in range(pieces):
            part = pl.ds(p * rows, rows)
            pltpu.make_async_copy(src.at[part, :], dst.at[part, :], sems.at[i]).start()
    for i in range(count):
        pltpu.make_async_copy(refs[i], refs[count + i], sems.at[i]).wait()


def per_device(
    out_grad, route_ids, route_weight, expert_inputs, gate_weight, up_weight, down_weight,
    out_gate, in_gate, values, conv_out, conv_taps, proj_weight,
):
    sds = jax.ShapeDtypeStruct
    hbm = pl.BlockSpec(memory_space=pltpu.HBM)
    vm = pltpu.VMEM
    dma = pltpu.SemaphoreType.DMA
    act = (TOK, CH)
    vmem = pl.BlockSpec(memory_space=pltpu.VMEM)
    shapes = [
        sds(act, BF), sds(act, BF), sds(act, BF), sds(act, BF), sds((ROWS, CH), F32),
        sds((TP * CH, HID), BF), sds((TP * CH, HID), BF), sds((HID, TP * CH), BF),
    ]
    outs = pl.pallas_call(
        layer_kernel,
        in_specs=[hbm] * 13,
        out_specs=[vmem] * 8,
        out_shape=[vm(o.shape, o.dtype) for o in shapes],
        scratch_shapes=[
            vm((2, TOK), jnp.int32), vm((2, TOK), F32), vm(act, BF), vm((SLOTS, TP * CH), BF),
            vm((TP * CH, 2 * HID), BF), vm((HID, TP * CH), BF), vm(act, BF), vm(act, BF), vm(act, BF),
            vm(act, BF), vm((3, CH), BF), vm((TP * CH, CH), BF),
            vm(act, BF), vm((SLOTS, TOK), BF), vm((SLOTS, TOK), F32), vm((SLOTS, CH), BF),
            vm((SLOTS, CH), BF), vm((TP, SLOTS, CH), BF), vm((SLOTS, HID), F32), vm((SLOTS, HID), F32),
            vm((SLOTS, HID), BF), vm((SLOTS, 2 * HID), BF),
            vm((TP, SLOTS, CH), BF), vm((2, SLOTS, CH), BF), vm((SLOTS, CH), BF), vm((SLOTS, CH), BF),
            vm((SLOTS, CH), BF), vm(act, BF), vm(act, BF), vm(act, BF), vm(act, BF),
            vm((TP,) + act, BF), vm(act, BF), vm((16, CH), BF), vm((16, CH), BF),
            vm((C, Z, Y) + act, BF), vm((TP, Y, C, ROWS, TOK), BF), vm((SP, ROWS, TOK), BF),
            dma((9,)), dma((2,)), dma((2,)), dma((Z + 1,)), dma((2,)), dma((1,)), dma((2,)),
            dma((1,)), dma((Z,)), dma((2,)), dma((2,)), dma((2,)), dma((1,)), dma((1,)), dma((Y,)),
            dma((2,)), dma((1,)), dma((4,)), dma((2,)), dma((1,)), dma((Z,)),
        ],
        compiler_params=pltpu.CompilerParams(
            collective_id=0, has_side_effects=True, vmem_limit_bytes=52428800
        ),
    )(
        route_ids.T, route_weight.T, out_grad, expert_inputs[0], gate_weight[0], up_weight[0],
        down_weight[0], out_gate, in_gate, values, conv_out, conv_taps, proj_weight,
    )
    resid, ogg, igg, vg, proj, gate_grad, up_grad, down_grad = pl.pallas_call(
        flush_kernel,
        in_specs=[vmem] * 8,
        out_specs=[hbm] * 8,
        out_shape=shapes,
        scratch_shapes=[dma((8,))],
        compiler_params=pltpu.CompilerParams(vmem_limit_bytes=1024 * 1024),
    )(*outs)
    return resid, ogg, igg, vg, proj, gate_grad[None], up_grad[None], down_grad[None]


def solution(mesh):
    return jax.shard_map(
        per_device,
        mesh=mesh,
        in_specs=(
            P("sp", "tp"), P("sp", None), P("sp", None), P("sp", None, None), P("sp", None, "tp"),
            P("sp", None, "tp"), P("sp", "tp", None), P("sp", "tp"), P("sp", "tp"), P("sp", "tp"),
            P("sp", "tp"), P(None, "tp"), P(None, "tp"),
        ),
        out_specs=(
            P("sp", "tp"), P("sp", "tp"), P("sp", "tp"), P("sp", "tp"), P("sp", "tp"),
            P("sp", None, "tp"), P("sp", None, "tp"), P("sp", "tp", None),
        ),
        check_vma=False,
    )
```
